256 devices in a mesh: grp: 2 (over y), sp: 16 (over z), fs: 4 (over x), tp: 2 (over core).
Axes of the slice: x: 4, y: 2, z: 16, core: 2. Of those that a mesh axis runs over, the one named last changes fastest.
The devices are a block of a 4x16x16 slice.
Arguments:
- tokens: bfloat16 [8, 2048, 2048], P(('grp', 'fs'), 'sp', 'tp'), parts along dimension 0, may hold values from -120 to 120
- mix_gain: float32 [2048], replicated, may hold values from 0.1 to 1.9
- attn_query: bfloat16 [2048, 1024], P('fs', 'tp'), may hold values from -0.375 to 0.375
- attn_key: bfloat16 [2048, 1024], P('fs', 'tp'), may hold values from -0.125 to 0.125
- attn_value: bfloat16 [2048, 1024], P('fs', 'tp'), may hold values from -0.125 to 0.125
- rec_query: bfloat16 [2048, 1024], P('fs', 'tp'), may hold values from -0.125 to 0.125
- rec_forget: bfloat16 [2048, 1024], P('fs', 'tp'), may hold values from -0.125 to 0.125
- rec_input: bfloat16 [2048, 1024], P('fs', 'tp'), may hold values from -0.125 to 0.125
- break_offset: float32 [8], P('tp'), may hold values from -13.5 to -7
- forget_room: float32 [8, 128], P('tp'), may hold values from 0.00024414062 to 0.05
- out_gain: float32 [128], replicated, may hold values from 0.1 to 1.9
- out_attn: bfloat16 [1024, 2048], P('tp', 'fs'), may hold values from -0.125 to 0.125
- out_rec: bfloat16 [1024, 2048], P('tp', 'fs'), may hold values from -0.125 to 0.125
Outputs:
- mixed: bfloat16 [8, 2048, 2048], P(('grp', 'fs'), ('sp', 'tp')), parts along dimension 0
The draws below stay inside these ranges and needn't reach their ends.
There are 2 independent parts, one for each index of `grp`. The reference program is written for one: setup_inputs(seed, part) draws one part's arguments, and reference() takes and returns one part's arrays. A program takes and returns all parts, laid end to end along the dimension named above; an argument that names none is the same for every part. Nothing has to cross between parts.
All inputs are finite; a program needn't handle non-finite values.
Results may differ from the reference program's by a relative error of at most 0.019.
Values may be sent and summed in bfloat16 or wider, within the bound.
No kernel may reach another device: no remote copies, remote signals or barrier semaphores. Data moves between devices by JAX's collectives and lax.ppermute only.
A program may use at most 64 MiB of HBM per device.

```python
import math
import jax
import jax.numpy as jnp
from jax import lax

D = 2048
SB_HEADS = 8
HEAD = 128
REC_HEADS = 8
DK = 128
DV = 128
REC_BLOCK = 64
TOK_DEV = 128
SEQS = 4
LENGTH = 2048
N_TP = 2


def draw_tokens(key, part):
    full_shape = (SEQS, LENGTH, D)
    subkeys = jax.random.split(key, 4)
    row_scale = jnp.exp(jax.random.uniform(subkeys[0], (SEQS, LENGTH, 1), jnp.float32, 0.0, math.log(10.0)))
    col_scale = jnp.exp(jax.random.uniform(subkeys[1], (1, 1, D), jnp.float32, 0.0, math.log(10.0)))
    regions = jax.random.normal(subkeys[2], (SEQS, LENGTH // TOK_DEV, 1, D), jnp.float32)
    regions = jnp.broadcast_to(regions, (SEQS, LENGTH // TOK_DEV, TOK_DEV, D)).reshape(full_shape)
    rough_part = jax.random.normal(subkeys[3], full_shape, jnp.float32)
    regions = 0.5 * regions
    drawn = (rough_part * col_scale / 3.0 + regions) * row_scale
    return jnp.clip(drawn, -120.0, 120.0).astype(jnp.bfloat16)


def block_scale(key, extent, shards, smallest, high):
    level, own = 1.0, jax.random.fold_in(key, 6)
    for position, blocks in shards:
        heights = jnp.exp(jax.random.uniform(jax.random.fold_in(own, position), (blocks,), jnp.float32, smallest / len(shards), high / len(shards)))
        level = level * jnp.repeat(heights, extent[position] // blocks).reshape([-1 if axis == position else 1 for axis in range(len(extent))])
    return level


def normal_values(stream_key, shape, width, bound, cuts=(), kind=jnp.bfloat16):
    entries = jax.random.normal(stream_key, shape, jnp.float32) * width
    if len(cuts) > 0:
        entries = block_scale(stream_key, shape, cuts, -0.22, 0.18) * entries
    return jnp.clip(entries, min=-bound, max=bound).astype(kind)


def setup_inputs(seed: int = 0, part: int = 0) -> dict:
    arg_keys = jax.random.split(jax.random.key(seed), 14)
    part_keys = jax.random.split(jax.random.fold_in(arg_keys[13], part), 14)
    tokens = draw_tokens(jax.random.fold_in(jax.random.fold_in(arg_keys[13], part), 71), part)
    mix_gain = jnp.clip(1.0 + 0.18 * jax.random.normal(arg_keys[1], (D,), jnp.float32), 0.1, 1.9)
    attn_query = normal_values(arg_keys[2], (D, SB_HEADS * HEAD), (D // 9) ** -0.5, 0.375, ((0, 4), (1, 2)))
    attn_key = normal_values(arg_keys[3], (D, SB_HEADS * HEAD), D ** -0.5, 0.125, ((0, 4), (1, 2)))
    attn_value = normal_values(arg_keys[4], (D, SB_HEADS * HEAD), D ** -0.5, 0.125, ((0, 4), (1, 2)))
    rec_query = normal_values(arg_keys[5], (D, REC_HEADS * DK), D ** -0.5, 0.125, ((0, 4), (1, 2)))
    rec_forget = normal_values(arg_keys[6], (D, REC_HEADS * DK), D ** -0.5, 0.125, ((0, 4), (1, 2)))
    rec_input = normal_values(arg_keys[7], (D, REC_HEADS * DV), D ** -0.5, 0.125, ((0, 4), (1, 2)))
    break_offset = jnp.clip(-13.5 + 6.5 * jax.random.uniform(arg_keys[8], (SB_HEADS,), jnp.float32) ** block_scale(arg_keys[8], (SB_HEADS,), ((0, 2),), -0.2, 0.2), -13.5, -7.0)
    forget_room = jnp.clip(jnp.exp(math.log(0.05) - 5.322034 * jax.random.uniform(arg_keys[9], (REC_HEADS, DK), jnp.float32) ** block_scale(arg_keys[9], (REC_HEADS, DK), ((0, 2),), -0.2, 0.2)), 0.00024414062, 0.05)
    out_gain = jnp.clip(1.0 + 0.18 * jax.random.normal(arg_keys[10], (DV,), jnp.float32), 0.1, 1.9)
    out_attn = normal_values(arg_keys[11], (SB_HEADS * HEAD, D), (SB_HEADS * HEAD + REC_HEADS * DV) ** -0.5, 0.125, ((0, 2), (1, 4)))
    out_rec = normal_values(arg_keys[12], (REC_HEADS * DV, D), (SB_HEADS * HEAD + REC_HEADS * DV) ** -0.5, 0.125, ((0, 2), (1, 4)))
    return {"tokens": tokens, "mix_gain": mix_gain, "attn_query": attn_query, "attn_key": attn_key, "attn_value": attn_value, "rec_query": rec_query, "rec_forget": rec_forget, "rec_input": rec_input, "break_offset": break_offset, "forget_room": forget_room, "out_gain": out_gain, "out_attn": out_attn, "out_rec": out_rec}


norm_eps = 1e-06
highest = lax.Precision.HIGHEST

def block_step(states, inputs):
    queries, key_in, value_rows, log_forget = inputs
    block_len = queries.shape[-2]
    cum_log = jnp.cumsum(log_forget, axis=-2)
    last_log = cum_log[..., -1:, :]
    q_dec = queries * jnp.exp(cum_log)
    k_inv = key_in * jnp.exp(-cum_log)
    causal = lax.iota(jnp.int32, block_len)[:, None] >= lax.iota(jnp.int32, block_len)[None, :]
    carried_part = jnp.einsum('...tk,...kv->...tv', q_dec, states, precision=highest)
    scores = jnp.where(causal, jnp.einsum('...tk,...sk->...ts', q_dec, k_inv, precision=highest), 0.0)
    inner_part = jnp.einsum('...ts,...sv->...tv', scores, value_rows, precision=highest)
    fresh_state = jnp.einsum('...sk,...sv->...kv', key_in * jnp.exp(last_log - cum_log), value_rows, precision=highest)
    return (jnp.exp(jnp.swapaxes(last_log, -1, -2)) * states + fresh_state, carried_part + inner_part)

def stick_sequence(queries, key_rows, value_rows, offsets):
    head_count = queries.shape[1]
    head_width = queries.shape[2]
    factor = 1.0 / math.sqrt(head_width)
    blocks = LENGTH // TOK_DEV

    def per_block(block_idx):
        q_blk = lax.dynamic_slice_in_dim(queries, block_idx * TOK_DEV, TOK_DEV, 0).astype(jnp.float32)
        q_pos = block_idx * TOK_DEV + lax.iota(jnp.int32, TOK_DEV)

        def turn(step_idx, carried):
            sums_acc, running = carried
            source = block_idx - step_idx
            k_blk = lax.dynamic_slice_in_dim(key_rows, source * TOK_DEV, TOK_DEV, 0).astype(jnp.float32)
            v_blk = lax.dynamic_slice_in_dim(value_rows, source * TOK_DEV, TOK_DEV, 0).astype(jnp.float32)
            scores = jnp.einsum('qhe,khe->hqk', q_blk, k_blk) * factor + offsets[:, None, None]
            k_pos = source * TOK_DEV + lax.iota(jnp.int32, TOK_DEV)
            strict = k_pos[None, :] < q_pos[:, None]
            log_keep = jnp.where(strict, jax.nn.log_sigmoid(-scores), 0.0)
            inner_sum = lax.cumsum(log_keep, axis=2, reverse=True) - log_keep
            sticks = jnp.where(strict, jnp.exp(jax.nn.log_sigmoid(scores) + inner_sum), 0.0)
            sticks = lax.optimization_barrier(sticks.astype(jnp.bfloat16)).astype(jnp.float32)
            partial_value = jnp.einsum('hqk,khe->qhe', sticks, v_blk)
            sums_acc = sums_acc + partial_value * jnp.transpose(jnp.exp(running))[:, :, None]
            return (sums_acc, running + lax.optimization_barrier(jnp.sum(log_keep, axis=2)))
        start_state = (jnp.zeros((TOK_DEV, head_count, head_width), jnp.float32), jnp.zeros((head_count, TOK_DEV), jnp.float32))
        sums_acc, unused_run = lax.fori_loop(0, block_idx + 1, turn, start_state)
        return sums_acc.astype(jnp.bfloat16)
    result = lax.map(per_block, jnp.arange(blocks, dtype=jnp.int32))
    return result.reshape(LENGTH, head_count, head_width)

def recur_sequence(queries, gate_pre, inputs, rooms, gain):
    key_in = rooms * jax.nn.sigmoid(-gate_pre.astype(jnp.float32))
    log_forget = jnp.log1p(-key_in)
    head_count = queries.shape[1]
    blocks = LENGTH // REC_BLOCK

    def split_blocks(tensor):
        return jnp.transpose(tensor.reshape(blocks, REC_BLOCK, head_count, tensor.shape[2]), (0, 2, 1, 3))
    empty_state = jnp.zeros((head_count, DK, DV), jnp.float32)
    final_state, pieces = lax.scan(block_step, empty_state, (split_blocks(queries.astype(jnp.float32)), split_blocks(key_in), split_blocks(inputs.astype(jnp.float32)), split_blocks(log_forget)))
    raw_out = jnp.transpose(pieces, (0, 2, 1, 3)).reshape(LENGTH, head_count, DV)
    factor = lax.rsqrt(lax.optimization_barrier(jnp.mean(raw_out * raw_out, axis=2, keepdims=True)) + norm_eps)
    return (raw_out * factor * gain).astype(jnp.bfloat16)

def reference(tokens, mix_gain, attn_query, attn_key, attn_value, rec_query, rec_forget, rec_input, break_offset, forget_room, out_gain, out_attn, out_rec):
    rows32 = tokens.astype(jnp.float32)
    factor = lax.rsqrt(lax.optimization_barrier(jnp.mean(rows32 * rows32, axis=2, keepdims=True)) + norm_eps)
    normed = (rows32 * factor * mix_gain).astype(jnp.bfloat16).reshape(SEQS * LENGTH, D)

    def project(matrix, head_width):
        product = jnp.dot(normed, matrix, preferred_element_type=jnp.float32).astype(jnp.bfloat16)
        return product.reshape(SEQS, LENGTH, matrix.shape[1] // head_width, head_width)
    attn_q = project(attn_query, HEAD)
    attn_k = project(attn_key, HEAD)
    attn_v = project(attn_value, HEAD)
    rec_q = project(rec_query, DK)
    rec_f = project(rec_forget, DK)
    rec_i = project(rec_input, DV)
    attn_out = lax.map(lambda triple: stick_sequence(triple[0], triple[1], triple[2], break_offset), (attn_q, attn_k, attn_v))
    rec_out = lax.map(lambda triple: recur_sequence(triple[0], triple[1], triple[2], forget_room, out_gain), (rec_q, rec_f, rec_i))
    attn_flat = attn_out.reshape(SEQS * LENGTH, SB_HEADS * HEAD)
    rec_flat = rec_out.reshape(SEQS * LENGTH, REC_HEADS * DV)
    attn_part = SB_HEADS * HEAD // N_TP
    rec_part = REC_HEADS * DV // N_TP
    mixed = jnp.zeros((SEQS * LENGTH, D), jnp.float32)
    for group in range(N_TP):
        attn_slice = attn_flat[:, group * attn_part:(group + 1) * attn_part]
        rec_slice = rec_flat[:, group * rec_part:(group + 1) * rec_part]
        partial_value = jnp.dot(attn_slice, out_attn[group * attn_part:(group + 1) * attn_part], preferred_element_type=jnp.float32) + jnp.dot(rec_slice, out_rec[group * rec_part:(group + 1) * rec_part], preferred_element_type=jnp.float32)
        mixed = mixed + lax.optimization_barrier(partial_value.astype(jnp.bfloat16)).astype(jnp.float32)
    return mixed.astype(jnp.bfloat16).reshape(SEQS, LENGTH, D)
```

```python
import math

import jax
import jax.numpy as jnp
from jax import lax
from jax.experimental import pallas as pl
from jax.experimental.pallas import tpu as pltpu
from jax.sharding import PartitionSpec as P


HEAD = 128
NORM_EPS = 1e-06
LOG2E = 1.4426950408889634

f32 = jnp.float32
bf16 = jnp.bfloat16


def mm(a, b):
    return lax.dot_general(a, b, (((1,), (0,)), ((), ())), preferred_element_type=f32)


def mm_t(a, b):
    return lax.dot_general(a, b, (((1,), (1,)), ((), ())), preferred_element_type=f32)


def halves(x):
    top = x.astype(bf16)
    return top, (x - top.astype(f32)).astype(bf16)


def ring(size, step):
    return [(k, (k + step) % size) for k in range(size)]


def shift(x, axis, step):
    return lax.ppermute(x, axis, ring(lax.axis_size(axis), step))


def swap(x):
    return lax.ppermute(x, "tp", [(0, 1), (1, 0)])


def weights_kernel(where_ref, *refs):
    out_ref = refs[-1]
    count = (len(refs) - 1) // 2
    mine, sent = refs[:count], refs[count : 2 * count]
    rows = mine[0].shape[0]
    here = where_ref[0]
    for k in range(count):
        place = pl.multiple_of(where_ref[1 + k] * rows, rows)

        @pl.when(here == 1)
        def _():
            out_ref[pl.ds(place, rows), :] = mine[k][...]

        @pl.when(here == 0)
        def _():
            out_ref[pl.ds(place, rows), :] = sent[k][...]


def project_kernel(gain_ref, weight_ref, *refs):
    count = (len(refs) - 3) // 2
    near, far = refs[:count], refs[count : 2 * count]
    query_ref, pair_ref, norm_ref = refs[2 * count :]
    rows, half = near[0].shape
    gain_a = gain_ref[0:1, :]
    gain_b = gain_ref[1:2, :]
    for k in range(count):
        a = near[k][...].astype(f32)
        b = far[k][...].astype(f32)
        total = jnp.sum(a * a + b * b, axis=1, keepdims=True)
        factor = lax.rsqrt(total * (1.0 / (2 * half)) + NORM_EPS)
        norm_ref[k * rows : (k + 1) * rows, 0:half] = (a * factor * gain_a).astype(bf16)
        norm_ref[k * rows : (k + 1) * rows, half:] = (b * factor * gain_b).astype(bf16)
    product = mm(norm_ref[...], weight_ref[...]).astype(bf16)
    query_ref[...] = product[:, :HEAD]
    pair_ref[...] = product[:, HEAD:]


def stick_body(half, offset, q_ref, kv_ref, mask_ref, out_ref, acc_ref, carry_ref, rows, blocks):
    chunk = 256
    span = 2 * rows
    factor = LOG2E / math.sqrt(HEAD)
    offset = offset * LOG2E
    sums = mask_ref[...]
    acc_ref[...] = jnp.zeros(acc_ref.shape, f32)
    carry_ref[...] = jnp.zeros(carry_ref.shape, f32)
    strict = (
        lax.broadcasted_iota(jnp.int32, (rows, span), 1)
        < lax.broadcasted_iota(jnp.int32, (rows, span), 0) + half * rows
    )
    for block in reversed(range(blocks)):
        keys = kv_ref[block * span : (block + 1) * span, 0:HEAD]
        values = kv_ref[block * span : (block + 1) * span, HEAD:]
        start = block * rows
        while start < blocks * rows:
            stop = min(start + chunk, blocks * rows)
            own = slice(start, stop)
            z = mm_t(q_ref[own, :], keys) * factor + offset
            tail = jnp.log(1.0 + jnp.exp2(-jnp.abs(z))) * LOG2E
            drop = jnp.maximum(z, 0.0) + tail
            take = jnp.minimum(z, 0.0) - tail
            if start == block * rows:
                first = jnp.where(strict, drop[:rows], 0.0)
                drop = jnp.concatenate([first, drop[rows:]], 0) if stop - start > rows else first
            both = mm(jnp.concatenate(halves(drop), 1), sums)
            stick = jnp.exp2(take - both[:, :span] - carry_ref[own, :])
            if start == block * rows:
                first = jnp.where(strict, stick[:rows], 0.0)
                stick = jnp.concatenate([first, stick[rows:]], 0) if stop - start > rows else first
            acc_ref[own, :] += mm(stick.astype(bf16), values)
            carry_ref[own, :] += both[:, span:]
            start = stop
    for block in range(blocks):
        out_ref[block] = acc_ref[block * rows : (block + 1) * rows, :].astype(bf16)


def recur_body(half, room, gain, q_ref, kv_ref, tri_ref, out_ref, cum_ref, rows, blocks):
    span = 2 * rows
    tri = tri_ref[...]
    causal = (
        lax.broadcasted_iota(jnp.int32, (rows, span), 1)
        <= lax.broadcasted_iota(jnp.int32, (rows, span), 0) + half * rows
    )
    place = pl.multiple_of(half * rows, rows)
    state = jnp.zeros((HEAD, HEAD), f32)
    for block in range(blocks):
        gate = kv_ref[block * span : (block + 1) * span, 0:HEAD].astype(f32)
        values = kv_ref[block * span : (block + 1) * span, HEAD:]
        key_in = room / (1.0 + jnp.exp(gate))
        log_forget = jnp.log(1.0 - key_in)
        cum = mm(tri, jnp.concatenate(halves(log_forget), 0))
        last = cum[span - 1 : span, :]
        cum_ref[block] = cum
        own_cum = cum_ref[block, pl.ds(place, rows), :]
        q_dec = (q_ref[block * rows : (block + 1) * rows, :].astype(f32) * jnp.exp(own_cum)).astype(bf16)
        k_inv = (key_in * jnp.exp(-cum)).astype(bf16)
        k_end = (key_in * jnp.exp(last - cum)).astype(bf16)
        scores = jnp.where(causal, mm_t(q_dec, k_inv), 0.0).astype(bf16)
        raw = mm(scores, values) + mm_t(q_dec, state.astype(bf16))
        fresh = lax.dot_general(values, k_end, (((0,), (0,)), ((), ())), preferred_element_type=f32)
        state = state * jnp.exp(last) + fresh
        scale = lax.rsqrt(jnp.mean(raw * raw, axis=1, keepdims=True) + NORM_EPS)
        out_ref[block] = (raw * scale * gain).astype(bf16)


def mixer_kernel(where_ref, offset_ref, room_ref, gain_ref, sums_ref, tri_ref, *refs):
    groups = (len(refs) - 6) // 3
    queries, mine, other = refs[:groups], refs[groups : 2 * groups], refs[2 * groups : 3 * groups]
    out_ref, q_ref, kv_ref, acc_ref, carry_ref, cum_ref = refs[3 * groups :]
    blocks, rows, _ = out_ref.shape
    half = where_ref[0]
    place = where_ref[1]
    far = 0
    for g in range(groups):
        for k in range(queries[g].shape[0] // rows):
            block = (place + SLOTS[far]) % blocks
            far += 1
            own = slice(k * rows, (k + 1) * rows)
            q_ref[pl.ds(pl.multiple_of(block * rows, rows), rows), :] = queries[g][own, :]
            at = pl.multiple_of((2 * block + half) * rows, rows)
            kv_ref[pl.ds(at, rows), :] = mine[g][own, :]
            at = pl.multiple_of((2 * block + 1 - half) * rows, rows)
            kv_ref[pl.ds(at, rows), :] = other[g][own, :]

    @pl.when(where_ref[2] == 1)
    def _():
        stick_body(
            half, offset_ref[0], q_ref, kv_ref, sums_ref, out_ref, acc_ref, carry_ref, rows, blocks
        )

    @pl.when(where_ref[2] == 0)
    def _():
        recur_body(
            half, room_ref[...], gain_ref[...], q_ref, kv_ref, tri_ref, out_ref, cum_ref, rows, blocks
        )


def output_kernel(where_ref, heads_ref, *refs):
    out_ref = refs[-1]
    pieces = refs[:-1]
    count = len(pieces) // 4
    half = where_ref[0]
    each = pieces[0].shape[0] // HEAD
    width = pieces[0].shape[1]
    heads = heads_ref.shape[0] // 2
    rows = []
    for core in range(2):
        first = each * (half if core == 0 else 1 - half)
        for kind in range(2):
            rows.append(
                jnp.concatenate([heads_ref[kind * heads + first + k] for k in range(each)], 1)
            )
    for k in range(count):
        total = sum(mm(rows[n], pieces[4 * k + n][...]) for n in range(4))
        at = pl.multiple_of(where_ref[1 + k] * width, width)
        out_ref[:, pl.ds(at, width)] = total.astype(bf16)


SLOTS = (0, 1, 15, 2, 14, 3, 13, 4, 12, 5, 11, 6, 10, 7, 9, 8)
GROUP = 4

whole = pl.BlockSpec(memory_space=pltpu.VMEM)
scalar = pl.BlockSpec(memory_space=pltpu.SMEM)


def body(
    tokens,
    mix_gain,
    attn_query,
    attn_key,
    attn_value,
    rec_query,
    rec_forget,
    rec_input,
    break_offset,
    forget_room,
    out_gain,
    out_attn,
    out_rec,
):
    sp, fs, tp = (lax.axis_size(a) for a in ("sp", "fs", "tp"))
    z, x, t = (lax.axis_index(a) for a in ("sp", "fs", "tp"))
    own_heads = break_offset.shape[0]
    heads = own_heads * tp
    head = z % heads
    local = head % own_heads
    is_attn = (z < heads).astype(jnp.int32)
    holds = (head // own_heads == t).astype(jnp.int32)

    rows = tokens.shape[1] // tp
    half_width = tokens.shape[2]
    own = tokens[0]
    near = lax.dynamic_slice_in_dim(own, t * rows, rows, 0)
    far = swap(lax.dynamic_slice_in_dim(own, (1 - t) * rows, rows, 0))

    def columns(attn, rec):
        a = lax.dynamic_slice_in_dim(attn, local * HEAD, HEAD, 1)
        r = lax.dynamic_slice_in_dim(rec, local * HEAD, HEAD, 1)
        return jnp.where(is_attn == 1, a, r)

    piece = jnp.concatenate(
        [columns(attn_query, rec_query), columns(attn_key, rec_forget), columns(attn_value, rec_input)], 1
    )

    def holder(place):
        return place % heads // own_heads

    def at(place, row, core):
        return (place * fs + row) * tp + core

    gathered = [piece]
    for step in range(1, fs):
        pairs = [
            (at(p, (r + step) % fs, holder(p)), at(p, r, holder(p))) for p in range(sp) for r in range(fs)
        ]
        gathered.append(lax.ppermute(piece, ("sp", "fs", "tp"), pairs))
    pairs = [
        (at(p, r, holder(p)), at(p, r, 1 - holder(p))) for p in range(sp) for r in range(fs)
    ]
    sent = [lax.ppermute(g, ("sp", "fs", "tp"), pairs) for g in gathered]
    sources = [(x + step) % fs for step in range(fs)]
    per_half = fs // tp
    places = [
        jnp.where(s // per_half == t, 0, per_half) + s % per_half for s in sources
    ]
    weight = pl.pallas_call(
        weights_kernel,
        out_shape=jax.ShapeDtypeStruct((fs * piece.shape[0], piece.shape[1]), bf16),
        in_specs=[scalar] + [whole] * (2 * fs),
        out_specs=whole,
        name="head_weights",
    )(jnp.stack([holds] + places).astype(jnp.int32), *gathered, *sent)
    gain_pair = mix_gain.reshape(tp, half_width)
    gain_pair = jnp.where(t == 0, gain_pair, gain_pair[::-1])

    last = sp // 2
    near_blocks, far_blocks = {0: near}, {0: far}
    ahead = [near, far]
    behind = [near, far]
    for hop in range(1, last + 1):
        for k, store in enumerate((near_blocks, far_blocks)):
            if hop < last or k == 0:
                ahead[k] = shift(ahead[k], "sp", 1)
                store[sp - hop] = ahead[k]
            if hop < last or k == 1:
                behind[k] = shift(behind[k], "sp", -1)
                store[hop] = behind[k]

    queries, pairs_own, pairs_other = [], [], []
    for first in range(0, sp, GROUP):
        slots = SLOTS[first : first + GROUP]
        query, pair = pl.pallas_call(
            project_kernel,
            out_shape=(
                jax.ShapeDtypeStruct((GROUP * rows, HEAD), bf16),
                jax.ShapeDtypeStruct((GROUP * rows, 2 * HEAD), bf16),
            ),
            in_specs=[whole] * (2 + 2 * GROUP),
            out_specs=(whole, whole),
            scratch_shapes=[pltpu.VMEM((GROUP * rows, 2 * half_width), bf16)],
            name="project",
        )(gain_pair, weight, *[near_blocks[s] for s in slots], *[far_blocks[s] for s in slots])
        queries.append(query)
        pairs_own.append(pair)
        pairs_other.append(swap(pair))

    attn_l, attn_r = shift(out_attn, "fs", 1), shift(out_attn, "fs", -1)
    rec_l, rec_r = shift(out_rec, "fs", 1), shift(out_rec, "fs", -1)
    attn_o, rec_o = shift(attn_l, "fs", 1), shift(rec_r, "fs", -1)
    out_pieces = []
    for a, r in ((out_attn, out_rec), (attn_r, rec_r), (attn_o, rec_o), (attn_l, rec_l)):
        out_pieces += [a, r, swap(a), swap(r)]

    span = rows * tp
    params = jnp.concatenate([break_offset[:, None], forget_room], 1)
    params = lax.dynamic_slice_in_dim(params, local, 1, 0)
    params = jnp.where(holds == 1, params, lax.ppermute(params, ("sp", "fs", "tp"), pairs))
    offset = params[0, :1]
    room = params[:, 1:]
    later = jnp.arange(span)[:, None] > jnp.arange(span)[None, :]
    sums = jnp.concatenate([later.astype(bf16), jnp.ones((span, span), bf16)], 1)
    sums = jnp.concatenate([sums, sums], 0)
    tri = (jnp.arange(span)[:, None] >= jnp.arange(span)[None, :]).astype(bf16)
    tri = jnp.concatenate([tri, tri], 1)
    groups = sp // GROUP
    mixed_heads = pl.pallas_call(
        mixer_kernel,
        out_shape=jax.ShapeDtypeStruct((sp, rows, HEAD), bf16),
        in_specs=[scalar, scalar] + [whole] * (4 + 3 * groups),
        out_specs=whole,
        scratch_shapes=[
            pltpu.VMEM((sp * rows, HEAD), bf16),
            pltpu.VMEM((sp * span, 2 * HEAD), bf16),
            pltpu.VMEM((sp * rows, HEAD), f32),
            pltpu.VMEM((sp * rows, HEAD), f32),
            pltpu.VMEM((sp, span, HEAD), f32),
        ],
        name="mixer",
    )(
        jnp.stack([t, z, is_attn]).astype(jnp.int32),
        offset,
        room,
        out_gain[None, :],
        sums,
        tri,
        *queries,
        *pairs_own,
        *pairs_other,
    )

    arrived = lax.all_to_all(mixed_heads, "sp", split_axis=0, concat_axis=0, tiled=True)
    mixed = pl.pallas_call(
        output_kernel,
        out_shape=jax.ShapeDtypeStruct((rows, fs * out_attn.shape[1]), bf16),
        in_specs=[scalar] + [whole] * (1 + len(out_pieces)),
        out_specs=whole,
        name="output",
    )(jnp.stack([t] + sources).astype(jnp.int32), arrived, *out_pieces)
    return mixed[None]


def solution(mesh):
    placed = (
        P(("grp", "fs"), "sp", "tp"),
        P(),
        P("fs", "tp"),
        P("fs", "tp"),
        P("fs", "tp"),
        P("fs", "tp"),
        P("fs", "tp"),
        P("fs", "tp"),
        P("tp"),
        P("tp", None),
        P(),
        P("tp", "fs"),
        P("tp", "fs"),
    )
    return jax.shard_map(
        body,
        mesh=mesh,
        in_specs=placed,
        out_specs=P(("grp", "fs"), ("sp", "tp"), None),
        check_vma=False,
    )
```

```python
import math

import jax
import jax.numpy as jnp
from jax import lax
from jax.experimental import pallas as pl
from jax.experimental.pallas import tpu as pltpu
from jax.sharding import PartitionSpec as P


HEAD = 128
NORM_EPS = 1e-06
LOG2E = 1.4426950408889634

f32 = jnp.float32
bf16 = jnp.bfloat16


def mm(a, b):
    return lax.dot_general(a, b, (((1,), (0,)), ((), ())), preferred_element_type=f32)


def mm_t(a, b):
    return lax.dot_general(a, b, (((1,), (1,)), ((), ())), preferred_element_type=f32)


def halves(x):
    top = x.astype(bf16)
    return top, (x - top.astype(f32)).astype(bf16)


def ring(size, step):
    return [(k, (k + step) % size) for k in range(size)]


def shift(x, axis, step):
    return lax.ppermute(x, axis, ring(lax.axis_size(axis), step))


def swap(x):
    return lax.ppermute(x, "tp", [(0, 1), (1, 0)])


def prepare_kernel(*refs):
    attn, rec, out_attn, out_rec = refs[0:3], refs[3:6], refs[6], refs[7]
    piece_ref, out_ref, sems = refs[8:]
    _, local, is_attn = place_of_head()
    rows = out_attn.shape[0]
    stacked = [
        pltpu.make_async_copy(out_attn, out_ref.at[0:rows, :], sems.at[3]),
        pltpu.make_async_copy(out_rec, out_ref.at[rows:, :], sems.at[4]),
    ]

    def columns(sources):
        at = pl.ds(pl.multiple_of(local * HEAD, HEAD), HEAD)
        copies = [
            pltpu.make_async_copy(
                sources[k].at[:, at], piece_ref.at[:, k * HEAD : (k + 1) * HEAD], sems.at[k]
            )
            for k in range(3)
        ]
        for copy in copies:
            copy.start()
        for copy in copies:
            copy.wait()

    for copy in stacked:
        copy.start()

    @pl.when(is_attn)
    def _():
        columns(attn)

    @pl.when(jnp.logical_not(is_attn))
    def _():
        columns(rec)

    for copy in stacked:
        copy.wait()


def project_kernel(gain_ref, offset_ref, room_ref, *refs):
    fs = lax.axis_size("fs")
    weights, refs = refs[:fs], refs[fs:]
    query_ref, pair_ref, norm_ref = refs[-3:]
    count = (len(refs) - 3) // 2
    near, far = refs[:count], refs[count : 2 * count]
    rows, half = near[0].shape
    width = weights[0].shape[0]
    x, t = lax.axis_index("fs"), lax.axis_index("tp")
    gain_a = gain_ref[:, pl.ds(pl.multiple_of(t * half, half), half)]
    gain_b = gain_ref[:, pl.ds(pl.multiple_of((1 - t) * half, half), half)]
    at_a = pl.ds(pl.multiple_of(t * half, half), half)
    at_b = pl.ds(pl.multiple_of((1 - t) * half, half), half)
    for k in range(count):
        a = near[k][...].astype(f32)
        b = far[k][...].astype(f32)
        total = jnp.sum(a * a + b * b, axis=1, keepdims=True)
        factor = lax.rsqrt(total * (1.0 / (2 * half)) + NORM_EPS)
        own = slice(k * rows, (k + 1) * rows)
        norm_ref[own, at_a] = (a * factor * gain_a).astype(bf16)
        norm_ref[own, at_b] = (b * factor * gain_b).astype(bf16)
    product = 0.0
    for step in range(fs):
        source = (x + step) % fs
        at = pl.ds(pl.multiple_of(source * width, width), width)
        product += mm(norm_ref[:, at], weights[step][...])
    product = product.astype(bf16)
    query_ref[...] = product[:, :HEAD]
    pair_ref[0 : count * rows, :] = product[:, HEAD:]
    if pair_ref.shape[0] > count * rows:
        _, local, _ = place_of_head()
        offset = jnp.full((1, HEAD), offset_ref[local], f32)
        rest = jnp.concatenate([room_ref[pl.ds(local, 1), :], offset], 1)
        parts = []
        for _ in range(3):
            parts.append(rest.astype(bf16).astype(f32))
            rest = rest - parts[-1]
        extra = pair_ref.shape[0] - count * rows
        pad = jnp.zeros((extra - 3, 2 * HEAD), f32)
        pair_ref[count * rows :, :] = jnp.concatenate(parts + [pad], 0).astype(bf16)


def stick_body(half, offset, q_ref, kv_ref, mask_ref, out_ref, acc_ref, carry_ref, rows, blocks):
    chunk = 256
    span = 2 * rows
    factor = LOG2E / math.sqrt(HEAD)
    offset = offset * LOG2E
    acc_ref[...] = jnp.zeros(acc_ref.shape, f32)
    carry_ref[...] = jnp.zeros(carry_ref.shape, f32)
    strict = (
        lax.broadcasted_iota(jnp.int32, (rows, span), 1)
        < lax.broadcasted_iota(jnp.int32, (rows, span), 0) + half * rows
    )
    for block in reversed(range(blocks)):
        keys = kv_ref[block * span : (block + 1) * span, 0:HEAD]
        values = kv_ref[block * span : (block + 1) * span, HEAD:]
        start = block * rows
        while start < blocks * rows:
            stop = min(start + chunk, blocks * rows)
            own = slice(start, stop)
            z = mm_t(q_ref[own, :], keys) * factor + offset
            tail = jnp.log(1.0 + jnp.exp2(-jnp.abs(z))) * LOG2E
            drop = jnp.maximum(z, 0.0) + tail
            take = jnp.minimum(z, 0.0) - tail
            if start == block * rows:
                first = jnp.where(strict, drop[:rows], 0.0)
                drop = jnp.concatenate([first, drop[rows:]], 0) if stop - start > rows else first
            both = mm(jnp.concatenate(halves(drop), 1), mask_ref[...])
            stick = jnp.exp2(take - both[:, :span] - carry_ref[own, :])
            if start == block * rows:
                first = jnp.where(strict, stick[:rows], 0.0)
                stick = jnp.concatenate([first, stick[rows:]], 0) if stop - start > rows else first
            acc_ref[own, :] += mm(stick.astype(bf16), values)
            carry_ref[own, :] += both[:, span:]
            start = stop
    for block in range(blocks):
        out_ref[block] = acc_ref[block * rows : (block + 1) * rows, :].astype(bf16)


def recur_body(half, room, gain, q_ref, kv_ref, tri, out_ref, cum_ref, rows, blocks):
    span = 2 * rows
    causal = (
        lax.broadcasted_iota(jnp.int32, (rows, span), 1)
        <= lax.broadcasted_iota(jnp.int32, (rows, span), 0) + half * rows
    )
    place = pl.multiple_of(half * rows, rows)
    state = jnp.zeros((HEAD, HEAD), f32)
    for block in range(blocks):
        gate = kv_ref[block * span : (block + 1) * span, 0:HEAD].astype(f32)
        values = kv_ref[block * span : (block + 1) * span, HEAD:]
        key_in = room / (1.0 + jnp.exp(gate))
        log_forget = jnp.log(1.0 - key_in)
        cum = mm(tri, jnp.concatenate(halves(log_forget), 0))
        last = cum[span - 1 : span, :]
        cum_ref[block] = cum
        own_cum = cum_ref[block, pl.ds(place, rows), :]
        q_dec = (q_ref[block * rows : (block + 1) * rows, :].astype(f32) * jnp.exp(own_cum)).astype(bf16)
        k_inv = (key_in * jnp.exp(-cum)).astype(bf16)
        k_end = (key_in * jnp.exp(last - cum)).astype(bf16)
        scores = jnp.where(causal, mm_t(q_dec, k_inv), 0.0).astype(bf16)
        raw = mm(scores, values) + mm_t(q_dec, state.astype(bf16))
        fresh = lax.dot_general(values, k_end, (((0,), (0,)), ((), ())), preferred_element_type=f32)
        state = state * jnp.exp(last) + fresh
        scale = lax.rsqrt(jnp.mean(raw * raw, axis=1, keepdims=True) + NORM_EPS)
        out_ref[block] = (raw * scale * gain).astype(bf16)


def mixer_kernel(gain_ref, *refs):
    groups = (len(refs) - 7) // 3
    queries, mine, other = refs[:groups], refs[groups : 2 * groups], refs[2 * groups : 3 * groups]
    out_ref, q_ref, kv_ref, acc_ref, carry_ref, cum_ref, sums_ref = refs[3 * groups :]
    blocks, rows, _ = out_ref.shape
    span = 2 * rows
    place, half = lax.axis_index("sp"), lax.axis_index("tp")
    head, _, is_attn = place_of_head()
    far = 0
    for g in range(groups):
        for k in range(queries[g].shape[0] // rows):
            block = (place + SLOTS[far]) % blocks
            far += 1
            own = slice(k * rows, (k + 1) * rows)
            q_ref[pl.ds(pl.multiple_of(block * rows, rows), rows), :] = queries[g][own, :]
            at = pl.multiple_of((2 * block + half) * rows, rows)
            kv_ref[pl.ds(at, rows), :] = mine[g][own, :]
            at = pl.multiple_of((2 * block + 1 - half) * rows, rows)
            kv_ref[pl.ds(at, rows), :] = other[g][own, :]
    used = queries[0].shape[0]
    holds = holder_of(head) == half
    parts = jnp.where(
        holds, mine[0][used : used + 8, :].astype(f32), other[0][used : used + 8, :].astype(f32)
    )
    params = parts[0:1, :] + parts[1:2, :] + parts[2:3, :]
    room, offset = params[:, :HEAD], params[:, HEAD:]
    down = lax.broadcasted_iota(jnp.int32, (span, span), 0)
    across = lax.broadcasted_iota(jnp.int32, (span, span), 1)

    @pl.when(is_attn)
    def _():
        later = jnp.where(down > across, 1.0, 0.0).astype(bf16)
        for k in range(2):
            sums_ref[k * span : (k + 1) * span, 0:span] = later
            sums_ref[k * span : (k + 1) * span, span:] = jnp.ones((span, span), bf16)
        stick_body(half, offset, q_ref, kv_ref, sums_ref, out_ref, acc_ref, carry_ref, rows, blocks)

    @pl.when(jnp.logical_not(is_attn))
    def _():
        upto = jnp.where(down >= across, 1.0, 0.0).astype(bf16)
        tri = jnp.concatenate([upto, upto], 1)
        recur_body(half, room, gain_ref[...], q_ref, kv_ref, tri, out_ref, cum_ref, rows, blocks)


def output_kernel(heads_ref, *refs):
    out_ref = refs[-1]
    fs = lax.axis_size("fs")
    x, half = lax.axis_index("fs"), lax.axis_index("tp")
    mine, other = refs[:fs], refs[fs : 2 * fs]
    width = mine[0].shape[1]
    heads = heads_ref.shape[0] // 2
    each = heads // 2
    rows = []
    for core in range(2):
        first = each * (half if core == 0 else 1 - half)
        rows.append(
            jnp.concatenate(
                [heads_ref[kind * heads + first + k] for kind in range(2) for k in range(each)], 1
            )
        )
    for step in range(fs):
        total = mm(rows[0], mine[step][...]) + mm(rows[1], other[step][...])
        at = pl.multiple_of((x + step) % fs * width, width)
        out_ref[:, pl.ds(at, width)] = total.astype(bf16)


SLOTS = (0, 1, 15, 2, 14, 3, 13, 4, 12, 5, 11, 6, 10, 7, 9, 8)
GROUPS = (12, 4)
PARAM_ROWS = 16

whole = pl.BlockSpec(memory_space=pltpu.VMEM)
scalar = pl.BlockSpec(memory_space=pltpu.SMEM)
anywhere = pl.BlockSpec(memory_space=pl.ANY)


def place_of_head():
    heads = lax.axis_size("sp") // 2
    place = lax.axis_index("sp")
    head = place % heads
    return head, head % (heads // lax.axis_size("tp")), place < heads


def holder_of(head):
    return head // (lax.axis_size("sp") // 2 // lax.axis_size("tp"))


def body(
    tokens,
    mix_gain,
    attn_query,
    attn_key,
    attn_value,
    rec_query,
    rec_forget,
    rec_input,
    break_offset,
    forget_room,
    out_gain,
    out_attn,
    out_rec,
):
    sp, fs, tp = (lax.axis_size(a) for a in ("sp", "fs", "tp"))
    t = lax.axis_index("tp")
    head, _, _ = place_of_head()

    rows = tokens.shape[1] // tp
    half_width = tokens.shape[2]
    own = tokens[0]
    near = lax.dynamic_slice_in_dim(own, t * rows, rows, 0)
    far = swap(lax.dynamic_slice_in_dim(own, (1 - t) * rows, rows, 0))

    depth = attn_query.shape[0]
    piece, out_own = pl.pallas_call(
        prepare_kernel,
        out_shape=(
            jax.ShapeDtypeStruct((depth, 3 * HEAD), bf16),
            jax.ShapeDtypeStruct((2 * out_attn.shape[0], out_attn.shape[1]), bf16),
        ),
        in_specs=[anywhere] * 8,
        out_specs=(anywhere, anywhere),
        scratch_shapes=[pltpu.SemaphoreType.DMA((5,))],
        name="prepare",
    )(attn_query, attn_key, attn_value, rec_query, rec_forget, rec_input, out_attn, out_rec)
    piece = jnp.where(holder_of(head) == t, piece, swap(piece))
    weights = [piece] + [shift(piece, "fs", -step) for step in range(1, fs)]

    last = sp // 2
    near_blocks, far_blocks = {0: near}, {0: far}
    ahead = [near, far]
    behind = [near, far]
    for hop in range(1, last + 1):
        for k, store in enumerate((near_blocks, far_blocks)):
            if hop < last or k == 0:
                ahead[k] = shift(ahead[k], "sp", 1)
                store[sp - hop] = ahead[k]
            if hop < last or k == 1:
                behind[k] = shift(behind[k], "sp", -1)
                store[hop] = behind[k]

    queries, pairs_own, pairs_other = [], [], []
    first = 0
    for count in GROUPS:
        slots = SLOTS[first : first + count]
        extra = 0 if first else PARAM_ROWS
        first += count
        call = pl.pallas_call(
            project_kernel,
            out_shape=(
                jax.ShapeDtypeStruct((count * rows, HEAD), bf16),
                jax.ShapeDtypeStruct((count * rows + extra, 2 * HEAD), bf16),
            ),
            in_specs=[whole, scalar] + [whole] * (1 + fs + 2 * count),
            out_specs=(whole, whole),
            scratch_shapes=[pltpu.VMEM((count * rows, 2 * half_width), bf16)],
            name="project",
        )
        query, pair = call(
            mix_gain[None, :],
            break_offset,
            forget_room,
            *weights,
            *[near_blocks[s] for s in slots],
            *[far_blocks[s] for s in slots],
        )
        queries.append(query)
        pairs_own.append(pair)
        pairs_other.append(swap(pair))

    out_mine = [out_own] + [shift(out_own, "fs", -step) for step in range(1, fs)]
    out_other = [swap(p) for p in out_mine]

    span = rows * tp
    groups = len(GROUPS)
    mixed_heads = pl.pallas_call(
        mixer_kernel,
        out_shape=jax.ShapeDtypeStruct((sp, rows, HEAD), bf16),
        in_specs=[whole] * (1 + 3 * groups),
        out_specs=whole,
        scratch_shapes=[
            pltpu.VMEM((sp * rows, HEAD), bf16),
            pltpu.VMEM((sp * span, 2 * HEAD), bf16),
            pltpu.VMEM((sp * rows, HEAD), f32),
            pltpu.VMEM((sp * rows, HEAD), f32),
            pltpu.VMEM((sp, span, HEAD), f32),
            pltpu.VMEM((2 * span, 2 * span), bf16),
        ],
        name="mixer",
    )(out_gain[None, :], *queries, *pairs_own, *pairs_other)

    arrived = lax.all_to_all(mixed_heads, "sp", split_axis=0, concat_axis=0, tiled=True)
    mixed = pl.pallas_call(
        output_kernel,
        out_shape=jax.ShapeDtypeStruct((rows, fs * out_attn.shape[1]), bf16),
        in_specs=[whole] * (1 + 2 * fs),
        out_specs=whole,
        name="output",
    )(arrived, *out_mine, *out_other)
    return mixed[None]


def solution(mesh):
    placed = (
        P(("grp", "fs"), "sp", "tp"),
        P(),
        P("fs", "tp"),
        P("fs", "tp"),
        P("fs", "tp"),
        P("fs", "tp"),
        P("fs", "tp"),
        P("fs", "tp"),
        P("tp"),
        P("tp", None),
        P(),
        P("tp", "fs"),
        P("tp", "fs"),
    )
    return jax.shard_map(
        body,
        mesh=mesh,
        in_specs=placed,
        out_specs=P(("grp", "fs"), ("sp", "tp"), None),
        check_vma=False,
    )
```

```python
import math

import jax
import jax.numpy as jnp
from jax import lax
from jax.experimental import pallas as pl
from jax.experimental.pallas import tpu as pltpu
from jax.sharding import PartitionSpec as P


HEAD = 128
NORM_EPS = 1e-06
LOG2E = 1.4426950408889634

f32 = jnp.float32
bf16 = jnp.bfloat16


def mm(a, b):
    return lax.dot_general(a, b, (((1,), (0,)), ((), ())), preferred_element_type=f32)


def mm_t(a, b):
    return lax.dot_general(a, b, (((1,), (1,)), ((), ())), preferred_element_type=f32)


def halves(x):
    top = x.astype(bf16)
    return top, (x - top.astype(f32)).astype(bf16)


def ring(size, step):
    return [(k, (k + step) % size) for k in range(size)]


def shift(x, axis, step):
    return lax.ppermute(x, axis, ring(lax.axis_size(axis), step))


def swap(x):
    return lax.ppermute(x, "tp", [(0, 1), (1, 0)])


def prepare_kernel(*refs):
    attn, rec, out_attn, out_rec = refs[0:3], refs[3:6], refs[6], refs[7]
    pack_ref, wide_ref, sems = refs[8:]
    _, local, is_attn = place_of_head()
    rows = out_attn.shape[0]
    at = pl.ds(pl.multiple_of(local * HEAD, HEAD), HEAD)
    stacked = [
        pltpu.make_async_copy(out_attn, pack_ref.at[0:rows, :], sems.at[3]),
        pltpu.make_async_copy(out_rec, pack_ref.at[rows : 2 * rows, :], sems.at[4]),
    ]

    def columns(sources):
        copies = [
            pltpu.make_async_copy(sources[k].at[:, at], wide_ref.at[k], sems.at[k]) for k in range(3)
        ]
        for copy in copies:
            copy.start()
        for copy in copies:
            copy.wait()

    @pl.when(is_attn)
    def _():
        columns(attn)

    @pl.when(jnp.logical_not(is_attn))
    def _():
        columns(rec)

    for copy in stacked:
        copy.start()
    for k in range(3):
        first = 2 * rows + k * HEAD
        pack_ref[first : first + HEAD, :] = wide_ref[k].T
    for copy in stacked:
        copy.wait()


def project_kernel(gain_ref, offset_ref, room_ref, *refs):
    fs = lax.axis_size("fs")
    mine, other, refs = refs[:fs], refs[fs : 2 * fs], refs[2 * fs :]
    query_ref, pair_ref, token_ref, weight_ref, norm_ref, sems = refs[-6:]
    count = (len(refs) - 6) // 2
    near, far = refs[:count], refs[count : 2 * count]
    rows, half = near[0].shape
    width = weight_ref.shape[1]
    each = mine[0].shape[1]
    x, t = lax.axis_index("fs"), lax.axis_index("tp")
    head, local, _ = place_of_head()
    holds = holder_of(head) == t
    at_a = pl.ds(pl.multiple_of(t * half, half), half)
    at_b = pl.ds(pl.multiple_of((1 - t) * half, half), half)
    tokens = []
    for k in range(count):
        own = slice(k * rows, (k + 1) * rows)
        for n, (source, at) in enumerate(((near[k], at_a), (far[k], at_b))):
            tokens.append(
                pltpu.make_async_copy(source, token_ref.at[own, at], sems.at[2 * k + n])
            )
    for copy in tokens:
        copy.start()
    own_weights, other_weights = [
        [
            pltpu.make_async_copy(
                pieces[step].at[pl.ds(pieces[step].shape[0] - width, width), :], weight_ref.at[step], sems.at[2 * count + step]
            )
            for step in range(fs)
        ]
        for pieces in (mine, other)
    ]

    @pl.when(holds)
    def _():
        for copy in own_weights:
            copy.start()

    @pl.when(jnp.logical_not(holds))
    def _():
        for copy in other_weights:
            copy.start()

    group = 4
    gain = gain_ref[...]
    for k in range(0, count, group):
        for copy in tokens[2 * k : 2 * (k + group)]:
            copy.wait()
        own = slice(k * rows, (k + group) * rows)
        value = token_ref[own, :].astype(f32)
        total = jnp.sum(value * value, axis=1, keepdims=True)
        factor = lax.rsqrt(total * (1.0 / (2 * half)) + NORM_EPS)
        norm_ref[own, :] = (value * factor * gain).astype(bf16)
    product = 0.0
    for step in range(fs):
        own_weights[step].wait()
        at = pl.ds(pl.multiple_of((x + step) % fs * each, each), each)
        product += mm_t(norm_ref[:, at], weight_ref[step])
    product = product.astype(bf16)
    query_ref[...] = product[:, :HEAD]
    pair_ref[0 : count * rows, :] = product[:, HEAD:]
    offset = jnp.full((1, HEAD), offset_ref[local], f32)
    rest = jnp.concatenate([room_ref[pl.ds(local, 1), :], offset], 1)
    parts = []
    for _ in range(3):
        parts.append(rest.astype(bf16).astype(f32))
        rest = rest - parts[-1]
    extra = pair_ref.shape[0] - count * rows
    pad = jnp.zeros((extra - 3, 2 * HEAD), f32)
    pair_ref[count * rows :, :] = jnp.concatenate(parts + [pad], 0).astype(bf16)


def stick_body(half, offset, q_ref, kv_ref, mask_ref, out_ref, acc_ref, carry_ref, rows, blocks):
    chunk = 256
    span = 2 * rows
    factor = LOG2E / math.sqrt(HEAD)
    offset = offset * LOG2E
    acc_ref[...] = jnp.zeros(acc_ref.shape, f32)
    carry_ref[...] = jnp.zeros(carry_ref.shape, f32)
    strict = (
        lax.broadcasted_iota(jnp.int32, (rows, span), 1)
        < lax.broadcasted_iota(jnp.int32, (rows, span), 0) + half * rows
    )
    for block in reversed(range(blocks)):
        keys = kv_ref[block * span : (block + 1) * span, 0:HEAD]
        values = kv_ref[block * span : (block + 1) * span, HEAD:]
        start = block * rows
        while start < blocks * rows:
            stop = min(start + chunk, blocks * rows)
            own = slice(start, stop)
            z = mm_t(q_ref[own, :], keys) * factor + offset
            tail = jnp.log(1.0 + jnp.exp2(-jnp.abs(z))) * LOG2E
            drop = jnp.maximum(z, 0.0) + tail
            take = jnp.minimum(z, 0.0) - tail
            if start == block * rows:
                first = jnp.where(strict, drop[:rows], 0.0)
                drop = jnp.concatenate([first, drop[rows:]], 0) if stop - start > rows else first
            both = mm(jnp.concatenate(halves(drop), 1), mask_ref[...])
            stick = jnp.exp2(take - both[:, :span] - carry_ref[own, :])
            if start == block * rows:
                first = jnp.where(strict, stick[:rows], 0.0)
                stick = jnp.concatenate([first, stick[rows:]], 0) if stop - start > rows else first
            acc_ref[own, :] += mm(stick.astype(bf16), values)
            carry_ref[own, :] += both[:, span:]
            start = stop
    for block in range(blocks):
        out_ref[block] = acc_ref[block * rows : (block + 1) * rows, :].astype(bf16)


def recur_body(half, room, gain, q_ref, kv_ref, tri, out_ref, cum_ref, rows, blocks):
    span = 2 * rows
    causal = (
        lax.broadcasted_iota(jnp.int32, (rows, span), 1)
        <= lax.broadcasted_iota(jnp.int32, (rows, span), 0) + half * rows
    )
    place = pl.multiple_of(half * rows, rows)
    state = jnp.zeros((HEAD, HEAD), f32)
    for block in range(blocks):
        gate = kv_ref[block * span : (block + 1) * span, 0:HEAD].astype(f32)
        values = kv_ref[block * span : (block + 1) * span, HEAD:]
        key_in = room / (1.0 + jnp.exp(gate))
        log_forget = jnp.log(1.0 - key_in)
        cum = mm(tri, jnp.concatenate(halves(log_forget), 0))
        last = cum[span - 1 : span, :]
        cum_ref[block] = cum
        own_cum = cum_ref[block, pl.ds(place, rows), :]
        q_dec = (q_ref[block * rows : (block + 1) * rows, :].astype(f32) * jnp.exp(own_cum)).astype(bf16)
        k_inv = (key_in * jnp.exp(-cum)).astype(bf16)
        k_end = (key_in * jnp.exp(last - cum)).astype(bf16)
        scores = jnp.where(causal, mm_t(q_dec, k_inv), 0.0).astype(bf16)
        raw = mm(scores, values) + mm_t(q_dec, state.astype(bf16))
        fresh = lax.dot_general(values, k_end, (((0,), (0,)), ((), ())), preferred_element_type=f32)
        state = state * jnp.exp(last) + fresh
        scale = lax.rsqrt(jnp.mean(raw * raw, axis=1, keepdims=True) + NORM_EPS)
        out_ref[block] = (raw * scale * gain).astype(bf16)


def mixer_kernel(gain_ref, query_ref, mine_ref, other_ref, *refs):
    out_ref, q_ref, kv_ref, acc_ref, carry_ref, cum_ref, sums_ref = refs
    blocks, rows, _ = out_ref.shape
    span = 2 * rows
    place, half = lax.axis_index("sp"), lax.axis_index("tp")
    head, _, is_attn = place_of_head()
    for k in range(blocks):
        block = (place + k) % blocks
        own = slice(k * rows, (k + 1) * rows)
        q_ref[pl.ds(pl.multiple_of(block * rows, rows), rows), :] = query_ref[own, :]
        at = pl.multiple_of((2 * block + half) * rows, rows)
        kv_ref[pl.ds(at, rows), :] = mine_ref[own, :]
        at = pl.multiple_of((2 * block + 1 - half) * rows, rows)
        kv_ref[pl.ds(at, rows), :] = other_ref[own, :]
    used = blocks * rows
    holds = holder_of(head) == half
    parts = jnp.where(
        holds, mine_ref[used : used + 8, :].astype(f32), other_ref[used : used + 8, :].astype(f32)
    )
    params = parts[0:1, :] + parts[1:2, :] + parts[2:3, :]
    room, offset = params[:, :HEAD], params[:, HEAD:]
    down = lax.broadcasted_iota(jnp.int32, (span, span), 0)
    across = lax.broadcasted_iota(jnp.int32, (span, span), 1)

    @pl.when(is_attn)
    def _():
        later = jnp.where(down > across, 1.0, 0.0).astype(bf16)
        for k in range(2):
            sums_ref[k * span : (k + 1) * span, 0:span] = later
            sums_ref[k * span : (k + 1) * span, span:] = jnp.ones((span, span), bf16)
        stick_body(half, offset, q_ref, kv_ref, sums_ref, out_ref, acc_ref, carry_ref, rows, blocks)

    @pl.when(jnp.logical_not(is_attn))
    def _():
        upto = jnp.where(down >= across, 1.0, 0.0).astype(bf16)
        tri = jnp.concatenate([upto, upto], 1)
        recur_body(half, room, gain_ref[...], q_ref, kv_ref, tri, out_ref, cum_ref, rows, blocks)


def output_kernel(heads_ref, *refs):
    out_ref, weight_ref, sems = refs[-3:]
    fs = lax.axis_size("fs")
    x, half = lax.axis_index("fs"), lax.axis_index("tp")
    pieces = refs[:fs], refs[fs : 2 * fs]
    depth, width = weight_ref.shape[2:]
    copies = [
        [
            pltpu.make_async_copy(
                pieces[core][step].at[0:depth, :], weight_ref.at[step, core], sems.at[step, core]
            )
            for core in range(2)
        ]
        for step in range(fs)
    ]
    for step in range(fs):
        for copy in copies[step]:
            copy.start()
    heads = heads_ref.shape[0] // 2
    each = heads // 2
    sides = []
    for core in range(2):
        first = each * (half if core == 0 else 1 - half)
        sides.append(
            jnp.concatenate(
                [heads_ref[kind * heads + first + k] for kind in range(2) for k in range(each)], 1
            )
        )
    for step in range(fs):
        total = 0.0
        for core in range(2):
            copies[step][core].wait()
            total += mm(sides[core], weight_ref[step, core])
        at = pl.multiple_of((x + step) % fs * width, width)
        out_ref[:, pl.ds(at, width)] = total.astype(bf16)


PARAM_ROWS = 16

whole = pl.BlockSpec(memory_space=pltpu.VMEM)
scalar = pl.BlockSpec(memory_space=pltpu.SMEM)
anywhere = pl.BlockSpec(memory_space=pl.ANY)


def place_of_head():
    heads = lax.axis_size("sp") // 2
    place = lax.axis_index("sp")
    head = place % heads
    return head, head % (heads // lax.axis_size("tp")), place < heads


def holder_of(head):
    return head // (lax.axis_size("sp") // 2 // lax.axis_size("tp"))


def body(
    tokens,
    mix_gain,
    attn_query,
    attn_key,
    attn_value,
    rec_query,
    rec_forget,
    rec_input,
    break_offset,
    forget_room,
    out_gain,
    out_attn,
    out_rec,
):
    sp, fs, tp = (lax.axis_size(a) for a in ("sp", "fs", "tp"))
    t = lax.axis_index("tp")
    _, _, _ = place_of_head()

    rows = tokens.shape[1] // tp
    half_width = tokens.shape[2]
    own = tokens[0]
    near = lax.dynamic_slice_in_dim(own, t * rows, rows, 0)
    far = swap(lax.dynamic_slice_in_dim(own, (1 - t) * rows, rows, 0))

    depth, wide = out_attn.shape
    prepare = pl.pallas_call(
        prepare_kernel,
        out_shape=jax.ShapeDtypeStruct((2 * depth + 3 * HEAD, attn_query.shape[0]), bf16),
        in_specs=[anywhere] * 8,
        out_specs=whole,
        scratch_shapes=[
            pltpu.VMEM((3, attn_query.shape[0], HEAD), bf16),
            pltpu.SemaphoreType.DMA((5,)),
        ],
        name="prepare",
    )
    pack = prepare(
        attn_query, attn_key, attn_value, rec_query, rec_forget, rec_input, out_attn, out_rec
    )
    from_prev, from_next = shift(pack, "fs", 1), shift(pack, "fs", -1)
    far_columns = from_prev[2 * depth :]
    far_columns = shift(far_columns, "fs", 1)
    from_far = shift(from_prev, "fs", 1)
    other_own = swap(pack)
    other_next, other_prev = swap(from_next), swap(from_prev)
    other_columns = swap(far_columns)
    other_far = swap(from_far)
    mine = [pack, from_next, from_far, from_prev]
    other = [other_own, other_next, other_far, other_prev]

    last = sp // 2
    near_blocks, far_blocks = {0: near}, {0: far}
    ahead = [near, far]
    behind = [near, far]
    for hop in range(1, last + 1):
        for k, store in enumerate((near_blocks, far_blocks)):
            if hop < last or k == 0:
                ahead[k] = shift(ahead[k], "sp", 1)
                store[sp - hop] = ahead[k]
            if hop < last or k == 1:
                behind[k] = shift(behind[k], "sp", -1)
                store[hop] = behind[k]

    query, pair = pl.pallas_call(
        project_kernel,
        out_shape=(
            jax.ShapeDtypeStruct((sp * rows, HEAD), bf16),
            jax.ShapeDtypeStruct((sp * rows + PARAM_ROWS, 2 * HEAD), bf16),
        ),
        in_specs=[whole, scalar, whole] + [anywhere] * (2 * fs + 2 * sp),
        out_specs=(whole, whole),
        scratch_shapes=[
            pltpu.VMEM((sp * rows, 2 * half_width), bf16),
            pltpu.VMEM((fs, 3 * HEAD, pack.shape[1]), bf16),
            pltpu.VMEM((sp * rows, 2 * half_width), bf16),
            pltpu.SemaphoreType.DMA((2 * sp + fs,)),
        ],
        name="project",
    )(
        mix_gain[None, :],
        break_offset,
        forget_room,
        pack,
        from_next,
        far_columns,
        from_prev,
        other_own,
        other_next,
        other_columns,
        other_prev,
        *[near_blocks[s] for s in range(sp)],
        *[far_blocks[s] for s in range(sp)],
    )
    pair_other = swap(pair)

    span = rows * tp
    mixed_heads = pl.pallas_call(
        mixer_kernel,
        out_shape=jax.ShapeDtypeStruct((sp, rows, HEAD), bf16),
        in_specs=[whole] * 4,
        out_specs=whole,
        scratch_shapes=[
            pltpu.VMEM((sp * rows, HEAD), bf16),
            pltpu.VMEM((sp * span, 2 * HEAD), bf16),
            pltpu.VMEM((sp * rows, HEAD), f32),
            pltpu.VMEM((sp * rows, HEAD), f32),
            pltpu.VMEM((sp, span, HEAD), f32),
            pltpu.VMEM((2 * span, 2 * span), bf16),
        ],
        name="mixer",
    )(out_gain[None, :], query, pair, pair_other)

    arrived = lax.all_to_all(mixed_heads, "sp", split_axis=0, concat_axis=0, tiled=True)
    mixed = pl.pallas_call(
        output_kernel,
        out_shape=jax.ShapeDtypeStruct((rows, fs * out_attn.shape[1]), bf16),
        in_specs=[whole] + [anywhere] * (2 * fs),
        out_specs=whole,
        scratch_shapes=[
            pltpu.VMEM((fs, 2, 2 * depth, wide), bf16),
            pltpu.SemaphoreType.DMA((fs, 2)),
        ],
        name="output",
    )(arrived, *mine, *other)
    return mixed[None]


def solution(mesh):
    placed = (
        P(("grp", "fs"), "sp", "tp"),
        P(),
        P("fs", "tp"),
        P("fs", "tp"),
        P("fs", "tp"),
        P("fs", "tp"),
        P("fs", "tp"),
        P("fs", "tp"),
        P("tp"),
        P("tp", None),
        P(),
        P("tp", "fs"),
        P("tp", "fs"),
    )
    return jax.shard_map(
        body,
        mesh=mesh,
        in_specs=placed,
        out_specs=P(("grp", "fs"), ("sp", "tp"), None),
        check_vma=False,
    )
```

```python
import math

import jax
import jax.numpy as jnp
from jax import lax
from jax.experimental import pallas as pl
from jax.experimental.pallas import tpu as pltpu
from jax.sharding import PartitionSpec as P


HEAD = 128
NORM_EPS = 1e-06
LOG2E = 1.4426950408889634

f32 = jnp.float32
bf16 = jnp.bfloat16


def mm(a, b):
    return lax.dot_general(a, b, (((1,), (0,)), ((), ())), preferred_element_type=f32)


def mm_t(a, b):
    return lax.dot_general(a, b, (((1,), (1,)), ((), ())), preferred_element_type=f32)


def halves(x):
    top = x.astype(bf16)
    return top, (x - top.astype(f32)).astype(bf16)


def ring(size, step):
    return [(k, (k + step) % size) for k in range(size)]


def shift(x, axis, step):
    return lax.ppermute(x, axis, ring(lax.axis_size(axis), step))


def swap(x):
    return lax.ppermute(x, "tp", [(0, 1), (1, 0)])


def columns_kernel(*refs):
    attn, rec = refs[0:3], refs[3:6]
    out_ref, wide_ref, sems = refs[6:]
    _, local, is_attn = place_of_head()
    at = pl.ds(pl.multiple_of(local * HEAD, HEAD), HEAD)

    def columns(sources):
        copies = [
            pltpu.make_async_copy(sources[k].at[:, at], wide_ref.at[k], sems.at[k]) for k in range(3)
        ]
        for copy in copies:
            copy.start()
        for copy in copies:
            copy.wait()

    @pl.when(is_attn)
    def _():
        columns(attn)

    @pl.when(jnp.logical_not(is_attn))
    def _():
        columns(rec)

    for k in range(3):
        out_ref[k * HEAD : (k + 1) * HEAD, :] = wide_ref[k].T


def pack_kernel(mine_ref, other_ref, out_attn, out_rec, pack_ref, sems):
    rows = out_attn.shape[0]
    copies = [
        pltpu.make_async_copy(out_attn, pack_ref.at[0:rows, :], sems.at[0]),
        pltpu.make_async_copy(out_rec, pack_ref.at[rows : 2 * rows, :], sems.at[1]),
    ]
    for copy in copies:
        copy.start()
    head, _, _ = place_of_head()
    holds = holder_of(head) == lax.axis_index("tp")

    @pl.when(holds)
    def _():
        pack_ref[2 * rows :, :] = mine_ref[...]

    @pl.when(jnp.logical_not(holds))
    def _():
        pack_ref[2 * rows :, :] = other_ref[...]

    for copy in copies:
        copy.wait()


def project_kernel(gain_ref, offset_ref, room_ref, *refs):
    fs = lax.axis_size("fs")
    packs, refs = refs[:fs], refs[fs:]
    query_ref, pair_ref, token_ref, weight_ref, norm_ref, sems = refs[-6:]
    count = (len(refs) - 6) // 2
    near, far = refs[:count], refs[count : 2 * count]
    rows, half = near[0].shape
    width, each = weight_ref.shape[1:]
    above = packs[0].shape[0] - width
    x, t = lax.axis_index("fs"), lax.axis_index("tp")
    _, local, _ = place_of_head()
    at_a = pl.ds(pl.multiple_of(t * half, half), half)
    at_b = pl.ds(pl.multiple_of((1 - t) * half, half), half)
    for k in range(count):
        own = slice(k * rows, (k + 1) * rows)
        pltpu.make_async_copy(near[k], token_ref.at[own, at_a], sems.at[2 * k]).start()
        pltpu.make_async_copy(far[k], token_ref.at[own, at_b], sems.at[2 * k + 1]).start()
    weights = [
        pltpu.make_async_copy(
            packs[step].at[above : above + width, :], weight_ref.at[step], sems.at[2 * count + step]
        )
        for step in range(fs)
    ]
    for copy in weights:
        copy.start()
    gain = gain_ref[...]

    def normalize(k, _):
        own = pl.ds(pl.multiple_of(k * rows, rows), rows)
        pltpu.make_async_copy(near[0], token_ref.at[own, at_a], sems.at[2 * k]).wait()
        pltpu.make_async_copy(far[0], token_ref.at[own, at_b], sems.at[2 * k + 1]).wait()
        value = token_ref[own, :].astype(f32)
        total = jnp.sum(value * value, axis=1, keepdims=True)
        factor = lax.rsqrt(total * (1.0 / (2 * half)) + NORM_EPS)
        norm_ref[own, :] = (value * factor * gain).astype(bf16)
        return 0

    lax.fori_loop(0, count, normalize, 0)
    for copy in weights:
        copy.wait()
    group = 4 * rows

    def multiply(k, _):
        own = pl.ds(pl.multiple_of(k * group, group), group)
        product = 0.0
        for step in range(fs):
            at = pl.ds(pl.multiple_of((x + step) % fs * each, each), each)
            product += mm_t(norm_ref[own, at], weight_ref[step])
        product = product.astype(bf16)
        query_ref[own, :] = product[:, :HEAD]
        pair_ref[own, :] = product[:, HEAD:]
        return 0

    lax.fori_loop(0, count * rows // group, multiply, 0)
    offset = jnp.full((1, HEAD), offset_ref[local], f32)
    rest = jnp.concatenate([room_ref[pl.ds(local, 1), :], offset], 1)
    parts = []
    for _ in range(3):
        parts.append(rest.astype(bf16).astype(f32))
        rest = rest - parts[-1]
    extra = pair_ref.shape[0] - count * rows
    pad = jnp.zeros((extra - 3, 2 * HEAD), f32)
    pair_ref[count * rows :, :] = jnp.concatenate(parts + [pad], 0).astype(bf16)


def stick_body(half, offset, q_ref, kv_ref, sums_ref, out_ref, acc_ref, carry_ref, rows, blocks):
    tile = 4
    span = 2 * rows
    factor = LOG2E / math.sqrt(HEAD)
    offset = offset * LOG2E
    strict = (
        lax.broadcasted_iota(jnp.int32, (rows, span), 1)
        < lax.broadcasted_iota(jnp.int32, (rows, span), 0) + half * rows
    )

    def masked(value, diagonal):
        if not diagonal:
            return value
        first = jnp.where(strict, value[:rows], 0.0)
        return first if value.shape[0] == rows else jnp.concatenate([first, value[rows:]], 0)

    def keys_of(group, n):
        return pl.ds(pl.multiple_of((group * tile + n) * span, span), span)

    def pieces(group, n, queries, diagonal):
        z = mm_t(queries, kv_ref[keys_of(group, n), 0:HEAD]) * factor + offset
        tail = jnp.log(1.0 + jnp.exp2(-jnp.abs(z))) * LOG2E
        drop = masked(jnp.maximum(z, 0.0) + tail, diagonal)
        take = jnp.minimum(z, 0.0) - tail
        both = mm(jnp.concatenate(halves(drop), 1), sums_ref[...])
        return take - both[:, :span], both[:, span:]

    def query_tile(index, _):
        base = pl.multiple_of(index * (tile * rows), tile * rows)
        acc_ref[...] = jnp.zeros(acc_ref.shape, f32)
        carry_ref[...] = jnp.zeros(carry_ref.shape, f32)
        for n in reversed(range(tile)):
            queries = q_ref[pl.ds(base + n * rows, (tile - n) * rows), :]
            power, total = pieces(index, n, queries, True)
            stick = masked(jnp.exp2(power - carry_ref[n * rows :, :]), True)
            acc_ref[n * rows :, :] += mm(stick.astype(bf16), kv_ref[keys_of(index, n), HEAD:])
            carry_ref[n * rows :, :] += total

        def earlier(step, _):
            group = index - 1 - step
            queries = q_ref[pl.ds(base, tile * rows), :]
            carry = carry_ref[...]
            out = 0.0
            for n in reversed(range(tile)):
                power, total = pieces(group, n, queries, False)
                stick = jnp.exp2(power - carry)
                out += mm(stick.astype(bf16), kv_ref[keys_of(group, n), HEAD:])
                carry += total
            acc_ref[...] += out
            carry_ref[...] = carry
            return 0

        lax.fori_loop(0, index, earlier, 0)
        for n in range(tile):
            out_ref[index * tile + n] = acc_ref[n * rows : (n + 1) * rows, :].astype(bf16)
        return 0

    lax.fori_loop(0, blocks // tile, query_tile, 0)


def recur_body(half, room, gain, q_ref, kv_ref, tri, out_ref, cum_ref, rows, blocks):
    span = 2 * rows
    at_once = 4
    causal = (
        lax.broadcasted_iota(jnp.int32, (rows, span), 1)
        <= lax.broadcasted_iota(jnp.int32, (rows, span), 0) + half * rows
    )
    place = pl.multiple_of(half * rows, rows)

    def one_block(block, slot, state):
        keys = pl.ds(pl.multiple_of(block * span, span), span)
        gate = kv_ref[keys, 0:HEAD].astype(f32)
        values = kv_ref[keys, HEAD:]
        key_in = room / (1.0 + jnp.exp(gate))
        log_forget = jnp.log(1.0 - key_in)
        cum = mm(tri, jnp.concatenate(halves(log_forget), 0))
        last = cum[span - 1 : span, :]
        cum_ref[slot] = cum
        own_cum = cum_ref[slot, pl.ds(place, rows), :]
        queries = q_ref[pl.ds(pl.multiple_of(block * rows, rows), rows), :].astype(f32)
        q_dec = (queries * jnp.exp(own_cum)).astype(bf16)
        k_inv = (key_in * jnp.exp(-cum)).astype(bf16)
        k_end = (key_in * jnp.exp(last - cum)).astype(bf16)
        scores = jnp.where(causal, mm_t(q_dec, k_inv), 0.0).astype(bf16)
        raw = mm(scores, values) + mm_t(q_dec, state.astype(bf16))
        fresh = lax.dot_general(values, k_end, (((0,), (0,)), ((), ())), preferred_element_type=f32)
        scale = lax.rsqrt(jnp.mean(raw * raw, axis=1, keepdims=True) + NORM_EPS)
        out_ref[block] = (raw * scale * gain).astype(bf16)
        return state * jnp.exp(last) + fresh

    def some_blocks(step, state):
        for slot in range(at_once):
            state = one_block(step * at_once + slot, slot, state)
        return state

    lax.fori_loop(0, blocks // at_once, some_blocks, jnp.zeros((HEAD, HEAD), f32))


def mixer_kernel(gain_ref, query_ref, mine_ref, other_ref, *refs):
    out_ref, q_ref, kv_ref, acc_ref, carry_ref, cum_ref, sums_ref = refs
    blocks, rows, _ = out_ref.shape
    span = 2 * rows
    place, half = lax.axis_index("sp"), lax.axis_index("tp")
    head, _, is_attn = place_of_head()
    for k in range(blocks):
        block = (place + k) % blocks
        own = slice(k * rows, (k + 1) * rows)
        q_ref[pl.ds(pl.multiple_of(block * rows, rows), rows), :] = query_ref[own, :]
        at = pl.multiple_of((2 * block + half) * rows, rows)
        kv_ref[pl.ds(at, rows), :] = mine_ref[own, :]
        at = pl.multiple_of((2 * block + 1 - half) * rows, rows)
        kv_ref[pl.ds(at, rows), :] = other_ref[own, :]
    used = blocks * rows
    holds = holder_of(head) == half
    parts = jnp.where(
        holds, mine_ref[used : used + 8, :].astype(f32), other_ref[used : used + 8, :].astype(f32)
    )
    params = parts[0:1, :] + parts[1:2, :] + parts[2:3, :]
    room, offset = params[:, :HEAD], params[:, HEAD:]
    down = lax.broadcasted_iota(jnp.int32, (span, span), 0)
    across = lax.broadcasted_iota(jnp.int32, (span, span), 1)

    @pl.when(is_attn)
    def _():
        later = jnp.where(down > across, 1.0, 0.0).astype(bf16)
        for k in range(2):
            sums_ref[k * span : (k + 1) * span, 0:span] = later
            sums_ref[k * span : (k + 1) * span, span:] = jnp.ones((span, span), bf16)
        stick_body(half, offset, q_ref, kv_ref, sums_ref, out_ref, acc_ref, carry_ref, rows, blocks)

    @pl.when(jnp.logical_not(is_attn))
    def _():
        upto = jnp.where(down >= across, 1.0, 0.0).astype(bf16)
        tri = jnp.concatenate([upto, upto], 1)
        recur_body(half, room, gain_ref[...], q_ref, kv_ref, tri, out_ref, cum_ref, rows, blocks)


def output_kernel(heads_ref, *refs):
    out_ref, weight_ref, sems = refs[-3:]
    fs = lax.axis_size("fs")
    x, half = lax.axis_index("fs"), lax.axis_index("tp")
    pieces = refs[:fs], refs[fs : 2 * fs]
    depth, width = weight_ref.shape[2:]
    copies = [
        [
            pltpu.make_async_copy(
                pieces[core][step].at[0:depth, :], weight_ref.at[step, core], sems.at[step, core]
            )
            for core in range(2)
        ]
        for step in range(fs)
    ]
    for step in range(fs):
        for copy in copies[step]:
            copy.start()
    heads = heads_ref.shape[0] // 2
    each = heads // 2
    sides = []
    for core in range(2):
        first = each * (half if core == 0 else 1 - half)
        sides.append(
            jnp.concatenate(
                [heads_ref[kind * heads + first + k] for kind in range(2) for k in range(each)], 1
            )
        )

    def column_block(step, _):
        total = 0.0
        for core in range(2):
            pltpu.make_async_copy(
                pieces[core][0].at[0:depth, :], weight_ref.at[step, core], sems.at[step, core]
            ).wait()
            total += mm(sides[core], weight_ref[step, core])
        at = pl.multiple_of((x + step) % fs * width, width)
        out_ref[:, pl.ds(at, width)] = total.astype(bf16)
        return 0

    lax.fori_loop(0, fs, column_block, 0)


PARAM_ROWS = 16

whole = pl.BlockSpec(memory_space=pltpu.VMEM)
scalar = pl.BlockSpec(memory_space=pltpu.SMEM)
anywhere = pl.BlockSpec(memory_space=pl.ANY)


def place_of_head():
    heads = lax.axis_size("sp") // 2
    place = lax.axis_index("sp")
    head = place % heads
    return head, head % (heads // lax.axis_size("tp")), place < heads


def holder_of(head):
    return head // (lax.axis_size("sp") // 2 // lax.axis_size("tp"))


def body(
    tokens,
    mix_gain,
    attn_query,
    attn_key,
    attn_value,
    rec_query,
    rec_forget,
    rec_input,
    break_offset,
    forget_room,
    out_gain,
    out_attn,
    out_rec,
):
    sp, fs, tp = (lax.axis_size(a) for a in ("sp", "fs", "tp"))
    t = lax.axis_index("tp")
    _, _, _ = place_of_head()

    rows = tokens.shape[1] // tp
    half_width = tokens.shape[2]
    own = tokens[0]
    near = lax.dynamic_slice_in_dim(own, t * rows, rows, 0)
    far = swap(lax.dynamic_slice_in_dim(own, (1 - t) * rows, rows, 0))

    depth, wide = out_attn.shape
    shape = jax.ShapeDtypeStruct((3 * HEAD, attn_query.shape[0]), bf16)
    pick = pl.pallas_call(
        columns_kernel,
        out_shape=shape,
        in_specs=[anywhere] * 6,
        out_specs=whole,
        scratch_shapes=[
            pltpu.VMEM((3, attn_query.shape[0], HEAD), bf16),
            pltpu.SemaphoreType.DMA((3,)),
        ],
        name="columns",
    )
    columns = pick(attn_query, attn_key, attn_value, rec_query, rec_forget, rec_input)
    columns_other = swap(columns)
    pack = pl.pallas_call(
        pack_kernel,
        out_shape=jax.ShapeDtypeStruct((2 * depth + shape.shape[0], wide), bf16),
        in_specs=[whole, whole, anywhere, anywhere],
        out_specs=whole,
        scratch_shapes=[pltpu.SemaphoreType.DMA((2,))],
        name="pack",
    )
    pack = pack(columns, columns_other, out_attn, out_rec)
    from_prev, from_next = shift(pack, "fs", 1), shift(pack, "fs", -1)
    from_far = shift(from_prev, "fs", 1)
    mine = [pack, from_next, from_far, from_prev]
    other = [swap(p) for p in mine]

    last = sp // 2
    near_blocks, far_blocks = {0: near}, {0: far}
    ahead = [near, far]
    behind = [near, far]
    for hop in range(1, last + 1):
        for k, store in enumerate((near_blocks, far_blocks)):
            if hop < last or k == 0:
                ahead[k] = shift(ahead[k], "sp", 1)
                store[sp - hop] = ahead[k]
            if hop < last or k == 1:
                behind[k] = shift(behind[k], "sp", -1)
                store[hop] = behind[k]

    query, pair = pl.pallas_call(
        project_kernel,
        out_shape=(
            jax.ShapeDtypeStruct((sp * rows, HEAD), bf16),
            jax.ShapeDtypeStruct((sp * rows + PARAM_ROWS, 2 * HEAD), bf16),
        ),
        in_specs=[whole, scalar, whole] + [anywhere] * (fs + 2 * sp),
        out_specs=(whole, whole),
        scratch_shapes=[
            pltpu.VMEM((sp * rows, 2 * half_width), bf16),
            pltpu.VMEM((fs, 3 * HEAD, pack.shape[1]), bf16),
            pltpu.VMEM((sp * rows, 2 * half_width), bf16),
            pltpu.SemaphoreType.DMA((2 * sp + fs,)),
        ],
        name="project",
    )(
        mix_gain[None, :],
        break_offset,
        forget_room,
        *mine,
        *[near_blocks[s] for s in range(sp)],
        *[far_blocks[s] for s in range(sp)],
    )
    pair_other = swap(pair)

    span = rows * tp
    mixed_heads = pl.pallas_call(
        mixer_kernel,
        out_shape=jax.ShapeDtypeStruct((sp, rows, HEAD), bf16),
        in_specs=[whole] * 4,
        out_specs=whole,
        scratch_shapes=[
            pltpu.VMEM((sp * rows, HEAD), bf16),
            pltpu.VMEM((sp * span, 2 * HEAD), bf16),
            pltpu.VMEM((4 * rows, HEAD), f32),
            pltpu.VMEM((4 * rows, HEAD), f32),
            pltpu.VMEM((4, span, HEAD), f32),
            pltpu.VMEM((2 * span, 2 * span), bf16),
        ],
        name="mixer",
    )(out_gain[None, :], query, pair, pair_other)

    arrived = lax.all_to_all(mixed_heads, "sp", split_axis=0, concat_axis=0, tiled=True)
    mixed = pl.pallas_call(
        output_kernel,
        out_shape=jax.ShapeDtypeStruct((rows, fs * out_attn.shape[1]), bf16),
        in_specs=[whole] + [anywhere] * (2 * fs),
        out_specs=whole,
        scratch_shapes=[
            pltpu.VMEM((fs, 2, 2 * depth, wide), bf16),
            pltpu.SemaphoreType.DMA((fs, 2)),
        ],
        name="output",
    )(arrived, *mine, *other)
    return mixed[None]


def solution(mesh):
    placed = (
        P(("grp", "fs"), "sp", "tp"),
        P(),
        P("fs", "tp"),
        P("fs", "tp"),
        P("fs", "tp"),
        P("fs", "tp"),
        P("fs", "tp"),
        P("fs", "tp"),
        P("tp"),
        P("tp", None),
        P(),
        P("tp", "fs"),
        P("tp", "fs"),
    )
    return jax.shard_map(
        body,
        mesh=mesh,
        in_specs=placed,
        out_specs=P(("grp", "fs"), ("sp", "tp"), None),
        check_vma=False,
    )
```

```python
import math

import jax
import jax.numpy as jnp
from jax import lax
from jax.experimental import pallas as pl
from jax.experimental.pallas import tpu as pltpu
from jax.sharding import PartitionSpec as P


HEAD = 128
NORM_EPS = 1e-06
LOG2E = 1.4426950408889634

f32 = jnp.float32
bf16 = jnp.bfloat16


def mm(a, b):
    return lax.dot_general(a, b, (((1,), (0,)), ((), ())), preferred_element_type=f32)


def mm_t(a, b):
    return lax.dot_general(a, b, (((1,), (1,)), ((), ())), preferred_element_type=f32)


def halves(x):
    top = x.astype(bf16)
    return top, (x - top.astype(f32)).astype(bf16)


def ring(size, step):
    return [(k, (k + step) % size) for k in range(size)]


def shift(x, axis, step):
    return lax.ppermute(x, axis, ring(lax.axis_size(axis), step))


def swap(x):
    return lax.ppermute(x, "tp", [(0, 1), (1, 0)])


def columns_kernel(*refs):
    attn, rec = refs[0:3], refs[3:6]
    out_ref, wide_ref, sems = refs[6:]
    _, local, is_attn = place_of_head()
    at = pl.ds(pl.multiple_of(local * HEAD, HEAD), HEAD)

    def columns(sources):
        copies = [
            pltpu.make_async_copy(sources[k].at[:, at], wide_ref.at[k], sems.at[k]) for k in range(3)
        ]
        for copy in copies:
            copy.start()
        for copy in copies:
            copy.wait()

    @pl.when(is_attn)
    def _():
        columns(attn)

    @pl.when(jnp.logical_not(is_attn))
    def _():
        columns(rec)

    for k in range(3):
        out_ref[k * HEAD : (k + 1) * HEAD, :] = wide_ref[k].T


def pack_kernel(mine_ref, other_ref, out_attn, out_rec, pack_ref, sems):
    rows = out_attn.shape[0]
    copies = [
        pltpu.make_async_copy(out_attn, pack_ref.at[0:rows, :], sems.at[0]),
        pltpu.make_async_copy(out_rec, pack_ref.at[rows : 2 * rows, :], sems.at[1]),
    ]
    for copy in copies:
        copy.start()
    head, _, _ = place_of_head()
    holds = holder_of(head) == lax.axis_index("tp")

    @pl.when(holds)
    def _():
        pack_ref[2 * rows :, :] = mine_ref[...]

    @pl.when(jnp.logical_not(holds))
    def _():
        pack_ref[2 * rows :, :] = other_ref[...]

    for copy in copies:
        copy.wait()


def project_kernel(gain_ref, offset_ref, room_ref, *refs):
    fs = lax.axis_size("fs")
    packs, refs = refs[:fs], refs[fs:]
    query_ref, pair_ref, norm_ref = refs[-3:]
    count = (len(refs) - 3) // 2
    near, far = refs[:count], refs[count : 2 * count]
    rows, half = near[0].shape
    each = packs[0].shape[1]
    x, t = lax.axis_index("fs"), lax.axis_index("tp")
    _, local, _ = place_of_head()
    at_a = pl.ds(pl.multiple_of(t * half, half), half)
    at_b = pl.ds(pl.multiple_of((1 - t) * half, half), half)
    for k in range(count):
        own = slice(k * rows, (k + 1) * rows)
        norm_ref[own, at_a] = near[k][...]
        norm_ref[own, at_b] = far[k][...]
    gain = gain_ref[...]

    def normalize(k, _):
        own = pl.ds(pl.multiple_of(k * rows, rows), rows)
        value = norm_ref[own, :].astype(f32)
        total = jnp.sum(value * value, axis=1, keepdims=True)
        factor = lax.rsqrt(total * (1.0 / (2 * half)) + NORM_EPS)
        norm_ref[own, :] = (value * factor * gain).astype(bf16)
        return 0

    lax.fori_loop(0, count, normalize, 0, unroll=2)
    group = 4 * rows

    def multiply(k, _):
        own = pl.ds(pl.multiple_of(k * group, group), group)
        product = 0.0
        for step in range(fs):
            at = pl.ds(pl.multiple_of((x + step) % fs * each, each), each)
            product += mm_t(norm_ref[own, at], packs[step][packs[step].shape[0] - 3 * HEAD :, :])
        product = product.astype(bf16)
        query_ref[own, :] = product[:, :HEAD]
        pair_ref[own, :] = product[:, HEAD:]
        return 0

    lax.fori_loop(0, count * rows // group, multiply, 0)
    offset = jnp.full((1, HEAD), offset_ref[local], f32)
    rest = jnp.concatenate([room_ref[pl.ds(local, 1), :], offset], 1)
    parts = []
    for _ in range(3):
        parts.append(rest.astype(bf16).astype(f32))
        rest = rest - parts[-1]
    extra = pair_ref.shape[0] - count * rows
    pad = jnp.zeros((extra - 3, 2 * HEAD), f32)
    pair_ref[count * rows :, :] = jnp.concatenate(parts + [pad], 0).astype(bf16)


def stick_body(half, offset, q_ref, kv_ref, sums_ref, out_ref, acc_ref, carry_ref, rows, blocks):
    tile = 4
    span = 2 * rows
    factor = LOG2E / math.sqrt(HEAD)
    offset = jnp.concatenate([offset * LOG2E] * tile, 1)
    strict = (
        lax.broadcasted_iota(jnp.int32, (rows, span), 1)
        < lax.broadcasted_iota(jnp.int32, (rows, span), 0) + half * rows
    )

    def keys_of(group):
        return pl.ds(pl.multiple_of(group * (tile * span), tile * span), tile * span)

    def attend(queries, group, carry, diagonal):
        keys = keys_of(group)
        z = mm_t(queries, kv_ref[keys, 0:HEAD]) * factor + offset
        tail = jnp.log(1.0 + jnp.exp2(-jnp.abs(z))) * LOG2E
        drop = jnp.maximum(z, 0.0) + tail
        take = jnp.minimum(z, 0.0) - tail
        parts = [None] * tile
        for n in reversed(range(tile)):
            across = slice(n * span, (n + 1) * span)
            skip = n * rows if diagonal else 0
            this = drop[skip:, across]
            if diagonal:
                first = jnp.where(strict, this[:rows], 0.0)
                this = jnp.concatenate([first, this[rows:]], 0) if n < tile - 1 else first
            both = mm(jnp.concatenate(halves(this), 1), sums_ref[...])
            stick = jnp.exp2(take[skip:, across] - both[:, :span] - carry[skip:])
            total = both[:, span:]
            if diagonal:
                first = jnp.where(strict, stick[:rows], 0.0)
                stick = jnp.concatenate([first, stick[rows:]], 0) if n < tile - 1 else first
            stick = stick.astype(bf16)
            if skip:
                stick = jnp.concatenate([jnp.zeros((skip, span), bf16), stick], 0)
                total = jnp.concatenate([jnp.zeros((skip, span), f32), total], 0)
            parts[n] = stick
            carry = carry + total
        return mm(jnp.concatenate(parts, 1), kv_ref[keys, HEAD:]), carry

    def query_tile(index, _):
        own = pl.ds(pl.multiple_of(index * (tile * rows), tile * rows), tile * rows)
        start = jnp.zeros((tile * rows, span), f32)
        acc_ref[...], carry_ref[...] = attend(q_ref[own, :], index, start, True)

        def earlier(step, _):
            out, carry = attend(q_ref[own, :], index - 1 - step, carry_ref[...], False)
            acc_ref[...] += out
            carry_ref[...] = carry
            return 0

        lax.fori_loop(0, index, earlier, 0)
        for n in range(tile):
            out_ref[index * tile + n] = acc_ref[n * rows : (n + 1) * rows, :].astype(bf16)
        return 0

    lax.fori_loop(0, blocks // tile, query_tile, 0)


def recur_body(half, room, gain, q_ref, kv_ref, tri, out_ref, cum_ref, rows, blocks):
    span = 2 * rows
    at_once = 2
    causal = (
        lax.broadcasted_iota(jnp.int32, (rows, span), 1)
        <= lax.broadcasted_iota(jnp.int32, (rows, span), 0) + half * rows
    )
    place = pl.multiple_of(half * rows, rows)

    def one_block(block, slot, state):
        keys = pl.ds(pl.multiple_of(block * span, span), span)
        gate = kv_ref[keys, 0:HEAD].astype(f32)
        values = kv_ref[keys, HEAD:]
        key_in = room / (1.0 + jnp.exp(gate))
        log_forget = jnp.log(1.0 - key_in)
        cum = mm(tri, jnp.concatenate(halves(log_forget), 0))
        last = cum[span - 1 : span, :]
        cum_ref[slot] = cum
        own_cum = cum_ref[slot, pl.ds(place, rows), :]
        queries = q_ref[pl.ds(pl.multiple_of(block * rows, rows), rows), :].astype(f32)
        q_dec = (queries * jnp.exp(own_cum)).astype(bf16)
        k_inv = (key_in * jnp.exp(-cum)).astype(bf16)
        k_end = (key_in * jnp.exp(last - cum)).astype(bf16)
        scores = jnp.where(causal, mm_t(q_dec, k_inv), 0.0).astype(bf16)
        raw = mm(scores, values) + mm_t(q_dec, state.astype(bf16))
        fresh = lax.dot_general(values, k_end, (((0,), (0,)), ((), ())), preferred_element_type=f32)
        scale = lax.rsqrt(jnp.mean(raw * raw, axis=1, keepdims=True) + NORM_EPS)
        out_ref[block] = (raw * scale * gain).astype(bf16)
        return state * jnp.exp(last) + fresh

    def some_blocks(step, state):
        for slot in range(at_once):
            state = one_block(step * at_once + slot, slot, state)
        return state

    lax.fori_loop(0, blocks // at_once, some_blocks, jnp.zeros((HEAD, HEAD), f32))


def mixer_kernel(gain_ref, query_ref, mine_ref, other_ref, *refs):
    out_ref, q_ref, kv_ref, acc_ref, carry_ref, cum_ref, sums_ref = refs
    blocks, rows, _ = out_ref.shape
    span = 2 * rows
    place, half = lax.axis_index("sp"), lax.axis_index("tp")
    head, _, is_attn = place_of_head()
    for k in range(blocks):
        block = (place + k) % blocks
        own = slice(k * rows, (k + 1) * rows)
        q_ref[pl.ds(pl.multiple_of(block * rows, rows), rows), :] = query_ref[own, :]
        at = pl.multiple_of((2 * block + half) * rows, rows)
        kv_ref[pl.ds(at, rows), :] = mine_ref[own, :]
        at = pl.multiple_of((2 * block + 1 - half) * rows, rows)
        kv_ref[pl.ds(at, rows), :] = other_ref[own, :]
    used = blocks * rows
    holds = holder_of(head) == half
    parts = jnp.where(
        holds, mine_ref[used : used + 8, :].astype(f32), other_ref[used : used + 8, :].astype(f32)
    )
    params = parts[0:1, :] + parts[1:2, :] + parts[2:3, :]
    room, offset = params[:, :HEAD], params[:, HEAD:]
    down = lax.broadcasted_iota(jnp.int32, (span, span), 0)
    across = lax.broadcasted_iota(jnp.int32, (span, span), 1)

    @pl.when(is_attn)
    def _():
        later = jnp.where(down > across, 1.0, 0.0).astype(bf16)
        for k in range(2):
            sums_ref[k * span : (k + 1) * span, 0:span] = later
            sums_ref[k * span : (k + 1) * span, span:] = jnp.ones((span, span), bf16)
        stick_body(half, offset, q_ref, kv_ref, sums_ref, out_ref, acc_ref, carry_ref, rows, blocks)

    @pl.when(jnp.logical_not(is_attn))
    def _():
        upto = jnp.where(down >= across, 1.0, 0.0).astype(bf16)
        tri = jnp.concatenate([upto, upto], 1)
        recur_body(half, room, gain_ref[...], q_ref, kv_ref, tri, out_ref, cum_ref, rows, blocks)


def output_kernel(heads_ref, *refs):
    out_ref = refs[-1]
    fs = lax.axis_size("fs")
    x, half = lax.axis_index("fs"), lax.axis_index("tp")
    pieces = refs[:fs], refs[fs : 2 * fs]
    width = pieces[0][0].shape[1]
    depth = heads_ref.shape[0] // 2 * HEAD
    heads = heads_ref.shape[0] // 2
    each = heads // 2
    sides = []
    for core in range(2):
        first = each * (half if core == 0 else 1 - half)
        sides.append(
            jnp.concatenate(
                [heads_ref[kind * heads + first + k] for kind in range(2) for k in range(each)], 1
            )
        )
    for step in range(fs):
        total = sum(mm(sides[core], pieces[core][step][0:depth, :]) for core in range(2))
        at = pl.multiple_of((x + step) % fs * width, width)
        out_ref[:, pl.ds(at, width)] = total.astype(bf16)


PARAM_ROWS = 16

MIB = 1 << 20


def limit(mib):
    return pltpu.CompilerParams(vmem_limit_bytes=mib * MIB)


def resident(arrays):
    return [pltpu.with_memory_space_constraint(a, pltpu.VMEM) for a in arrays]


def left_out(arrays):
    return [pltpu.with_memory_space_constraint(a, pltpu.HBM) for a in arrays]


whole = pl.BlockSpec(memory_space=pltpu.VMEM)
scalar = pl.BlockSpec(memory_space=pltpu.SMEM)
outside = pl.BlockSpec(memory_space=pltpu.HBM)


def place_of_head():
    heads = lax.axis_size("sp") // 2
    place = lax.axis_index("sp")
    head = place % heads
    return head, head % (heads // lax.axis_size("tp")), place < heads


def holder_of(head):
    return head // (lax.axis_size("sp") // 2 // lax.axis_size("tp"))


def body(
    tokens,
    mix_gain,
    attn_query,
    attn_key,
    attn_value,
    rec_query,
    rec_forget,
    rec_input,
    break_offset,
    forget_room,
    out_gain,
    out_attn,
    out_rec,
):
    sp, fs, tp = (lax.axis_size(a) for a in ("sp", "fs", "tp"))
    t = lax.axis_index("tp")
    _, _, _ = place_of_head()

    rows = tokens.shape[1] // tp
    half_width = tokens.shape[2]
    own = tokens[0]
    near = lax.dynamic_slice_in_dim(own, t * rows, rows, 0)
    far = swap(lax.dynamic_slice_in_dim(own, (1 - t) * rows, rows, 0))

    depth, wide = out_attn.shape
    shape = jax.ShapeDtypeStruct((3 * HEAD, attn_query.shape[0]), bf16)
    pick = pl.pallas_call(
        columns_kernel,
        out_shape=shape,
        in_specs=[outside] * 6,
        out_specs=whole,
        scratch_shapes=[
            pltpu.VMEM((3, attn_query.shape[0], HEAD), bf16),
            pltpu.SemaphoreType.DMA((3,)),
        ],
        compiler_params=limit(6),
        name="columns",
    )
    columns = pick(*left_out([attn_query, attn_key, attn_value, rec_query, rec_forget, rec_input]))
    columns_other = swap(columns)
    pack = pl.pallas_call(
        pack_kernel,
        out_shape=jax.ShapeDtypeStruct((2 * depth + shape.shape[0], wide), bf16),
        in_specs=[whole, whole, outside, outside],
        out_specs=whole,
        scratch_shapes=[pltpu.SemaphoreType.DMA((2,))],
        compiler_params=limit(8),
        name="pack",
    )
    pack = pack(*resident([columns, columns_other]), *left_out([out_attn, out_rec]))
    from_prev, from_next = shift(pack, "fs", 1), shift(pack, "fs", -1)
    far_columns = from_prev[2 * depth :]
    far_columns = shift(far_columns, "fs", 1)
    from_far = shift(from_prev, "fs", 1)
    mine = [pack, from_next, from_far, from_prev]
    other_own, other_next, other_prev = swap(pack), swap(from_next), swap(from_prev)
    other_far = swap(from_far)
    other = [other_own, other_next, other_far, other_prev]

    last = sp // 2
    near_blocks, far_blocks = {0: near}, {0: far}
    ahead = [near, far]
    behind = [near, far]
    for hop in range(1, last + 1):
        for k, store in enumerate((near_blocks, far_blocks)):
            if hop < last or k == 0:
                ahead[k] = shift(ahead[k], "sp", 1)
                store[sp - hop] = ahead[k]
            if hop < last or k == 1:
                behind[k] = shift(behind[k], "sp", -1)
                store[hop] = behind[k]

    query, pair = pl.pallas_call(
        project_kernel,
        out_shape=(
            jax.ShapeDtypeStruct((sp * rows, HEAD), bf16),
            jax.ShapeDtypeStruct((sp * rows + PARAM_ROWS, 2 * HEAD), bf16),
        ),
        in_specs=[whole, scalar] + [whole] * (1 + fs + 2 * sp),
        out_specs=(whole, whole),
        scratch_shapes=[pltpu.VMEM((sp * rows, 2 * half_width), bf16)],
        compiler_params=limit(12),
        name="project",
    )(
        mix_gain[None, :],
        break_offset,
        forget_room,
        *resident([pack, from_next, far_columns, from_prev]),
        *resident([near_blocks[s] for s in range(sp)]),
        *resident([far_blocks[s] for s in range(sp)]),
    )
    pair_other = swap(pair)

    span = rows * tp
    mixed_heads = pl.pallas_call(
        mixer_kernel,
        out_shape=jax.ShapeDtypeStruct((sp, rows, HEAD), bf16),
        in_specs=[whole] * 4,
        out_specs=whole,
        scratch_shapes=[
            pltpu.VMEM((sp * rows, HEAD), bf16),
            pltpu.VMEM((sp * span, 2 * HEAD), bf16),
            pltpu.VMEM((4 * rows, HEAD), f32),
            pltpu.VMEM((4 * rows, HEAD), f32),
            pltpu.VMEM((2, span, HEAD), f32),
            pltpu.VMEM((2 * span, 2 * span), bf16),
        ],
        compiler_params=limit(12),
        name="mixer",
    )(out_gain[None, :], *resident([query, pair, pair_other]))

    arrived = lax.all_to_all(mixed_heads, "sp", split_axis=0, concat_axis=0, tiled=True)
    mixed = pl.pallas_call(
        output_kernel,
        out_shape=jax.ShapeDtypeStruct((rows, fs * out_attn.shape[1]), bf16),
        in_specs=[whole] * (1 + 2 * fs),
        out_specs=whole,
        compiler_params=limit(16),
        name="output",
    )(*resident([arrived, *mine, *other]))
    return mixed[None]


def solution(mesh):
    placed = (
        P(("grp", "fs"), "sp", "tp"),
        P(),
        P("fs", "tp"),
        P("fs", "tp"),
        P("fs", "tp"),
        P("fs", "tp"),
        P("fs", "tp"),
        P("fs", "tp"),
        P("tp"),
        P("tp", None),
        P(),
        P("tp", "fs"),
        P("tp", "fs"),
    )
    return jax.shard_map(
        body,
        mesh=mesh,
        in_specs=placed,
        out_specs=P(("grp", "fs"), ("sp", "tp"), None),
        check_vma=False,
    )
```

```python
import functools
import math

import jax
import jax.numpy as jnp
from jax import lax
from jax.experimental import pallas as pl
from jax.experimental.pallas import tpu as pltpu
from jax.sharding import PartitionSpec as P


HEAD = 128
NORM_EPS = 1e-06
LOG2E = 1.4426950408889634

f32 = jnp.float32
bf16 = jnp.bfloat16


def mm(a, b):
    return lax.dot_general(a, b, (((1,), (0,)), ((), ())), preferred_element_type=f32)


def mm_t(a, b):
    return lax.dot_general(a, b, (((1,), (1,)), ((), ())), preferred_element_type=f32)


def halves(x):
    top = x.astype(bf16)
    return top, (x - top.astype(f32)).astype(bf16)


def ring(size, step):
    return [(k, (k + step) % size) for k in range(size)]


def shift(x, axis, step):
    return lax.ppermute(x, axis, ring(lax.axis_size(axis), step))


def swap(x):
    return lax.ppermute(x, "tp", [(0, 1), (1, 0)])


def columns_kernel(*refs):
    attn, rec = refs[0:3], refs[3:6]
    out_ref, wide_ref, sems = refs[6:]
    _, local, is_attn = place_of_head()
    at = pl.ds(pl.multiple_of(local * HEAD, HEAD), HEAD)

    def columns(sources):
        copies = [
            pltpu.make_async_copy(sources[k].at[:, at], wide_ref.at[k], sems.at[k]) for k in range(3)
        ]
        for copy in copies:
            copy.start()
        for copy in copies:
            copy.wait()

    @pl.when(is_attn)
    def _():
        columns(attn)

    @pl.when(jnp.logical_not(is_attn))
    def _():
        columns(rec)

    for k in range(3):
        out_ref[k * HEAD : (k + 1) * HEAD, :] = wide_ref[k].T


def pack_kernel(mine_ref, other_ref, out_attn, out_rec, pack_ref, sems):
    rows = out_attn.shape[0]
    copies = [
        pltpu.make_async_copy(out_attn, pack_ref.at[0:rows, :], sems.at[0]),
        pltpu.make_async_copy(out_rec, pack_ref.at[rows : 2 * rows, :], sems.at[1]),
    ]
    for copy in copies:
        copy.start()
    head, _, _ = place_of_head()
    holds = holder_of(head) == lax.axis_index("tp")

    @pl.when(holds)
    def _():
        pack_ref[2 * rows :, :] = mine_ref[...]

    @pl.when(jnp.logical_not(holds))
    def _():
        pack_ref[2 * rows :, :] = other_ref[...]

    for copy in copies:
        copy.wait()


def project_kernel(done, gain_ref, offset_ref, room_ref, *refs):
    fs = lax.axis_size("fs")
    query_ref, pair_ref, norm_ref = refs[-3:]
    if done:
        query_ref[0:done, :] = refs[0][...]
        pair_ref[0:done, :] = refs[1][...]
        refs = refs[2:]
    packs, refs = refs[:fs], refs[fs:]
    count = (len(refs) - 3) // 2
    near, far = refs[:count], refs[count : 2 * count]
    rows, half = near[0].shape
    each = packs[0].shape[1]
    x, t = lax.axis_index("fs"), lax.axis_index("tp")
    _, local, _ = place_of_head()
    at_a = pl.ds(pl.multiple_of(t * half, half), half)
    at_b = pl.ds(pl.multiple_of((1 - t) * half, half), half)
    for k in range(count):
        own = slice(k * rows, (k + 1) * rows)
        norm_ref[own, at_a] = near[k][...]
        norm_ref[own, at_b] = far[k][...]
    gain = gain_ref[...]

    def normalize(k, _):
        own = pl.ds(pl.multiple_of(k * rows, rows), rows)
        value = norm_ref[own, :].astype(f32)
        total = jnp.sum(value * value, axis=1, keepdims=True)
        factor = lax.rsqrt(total * (1.0 / (2 * half)) + NORM_EPS)
        norm_ref[own, :] = (value * factor * gain).astype(bf16)
        return 0

    lax.fori_loop(0, count, normalize, 0)
    group = 4 * rows

    def multiply(k, _):
        own = pl.ds(pl.multiple_of(k * group, group), group)
        product = 0.0
        for step in range(fs):
            at = pl.ds(pl.multiple_of((x + step) % fs * each, each), each)
            product += mm_t(norm_ref[own, at], packs[step][packs[step].shape[0] - 3 * HEAD :, :])
        product = product.astype(bf16)
        to = pl.ds(pl.multiple_of(done + k * group, group), group)
        query_ref[to, :] = product[:, :HEAD]
        pair_ref[to, :] = product[:, HEAD:]
        return 0

    lax.fori_loop(0, count * rows // group, multiply, 0)
    if not done:
        return
    offset = jnp.full((1, HEAD), offset_ref[local], f32)
    rest = jnp.concatenate([room_ref[pl.ds(local, 1), :], offset], 1)
    parts = []
    for _ in range(3):
        parts.append(rest.astype(bf16).astype(f32))
        rest = rest - parts[-1]
    used = done + count * rows
    pad = jnp.zeros((PARAM_ROWS - 3, 2 * HEAD), f32)
    pair_ref[used : used + PARAM_ROWS, :] = jnp.concatenate(parts + [pad], 0).astype(bf16)


def stick_body(half, offset, q_ref, kv_ref, sums_ref, out_ref, acc_ref, carry_ref, rows, blocks):
    tile = 4
    span = 2 * rows
    factor = LOG2E / math.sqrt(HEAD)
    offset = jnp.concatenate([offset * LOG2E] * tile, 1)
    strict = (
        lax.broadcasted_iota(jnp.int32, (rows, span), 1)
        < lax.broadcasted_iota(jnp.int32, (rows, span), 0) + half * rows
    )

    def keys_of(group):
        return pl.ds(pl.multiple_of(group * (tile * span), tile * span), tile * span)

    def attend(queries, group, carry, diagonal):
        keys = keys_of(group)
        z = mm_t(queries, kv_ref[keys, 0:HEAD]) * factor + offset
        tail = jnp.log(1.0 + jnp.exp2(-jnp.abs(z))) * LOG2E
        drop = jnp.maximum(z, 0.0) + tail
        take = jnp.minimum(z, 0.0) - tail
        parts = [None] * tile
        for n in reversed(range(tile)):
            across = slice(n * span, (n + 1) * span)
            skip = n * rows if diagonal else 0
            this = drop[skip:, across]
            if diagonal:
                first = jnp.where(strict, this[:rows], 0.0)
                this = jnp.concatenate([first, this[rows:]], 0) if n < tile - 1 else first
            both = mm(jnp.concatenate(halves(this), 1), sums_ref[...])
            stick = jnp.exp2(take[skip:, across] - both[:, :span] - carry[skip:])
            total = both[:, span:]
            if diagonal:
                first = jnp.where(strict, stick[:rows], 0.0)
                stick = jnp.concatenate([first, stick[rows:]], 0) if n < tile - 1 else first
            stick = stick.astype(bf16)
            if skip:
                stick = jnp.concatenate([jnp.zeros((skip, span), bf16), stick], 0)
                total = jnp.concatenate([jnp.zeros((skip, span), f32), total], 0)
            parts[n] = stick
            carry = carry + total
        return mm(jnp.concatenate(parts, 1), kv_ref[keys, HEAD:]), carry

    def query_tile(index, _):
        own = pl.ds(pl.multiple_of(index * (tile * rows), tile * rows), tile * rows)
        start = jnp.zeros((tile * rows, span), f32)
        acc_ref[...], carry_ref[...] = attend(q_ref[own, :], index, start, True)

        def earlier(step, _):
            out, carry = attend(q_ref[own, :], index - 1 - step, carry_ref[...], False)
            acc_ref[...] += out
            carry_ref[...] = carry
            return 0

        lax.fori_loop(0, index, earlier, 0)
        for n in range(tile):
            out_ref[index * tile + n] = acc_ref[n * rows : (n + 1) * rows, :].astype(bf16)
        return 0

    lax.fori_loop(0, blocks // tile, query_tile, 0)


def recur_body(half, room, gain, q_ref, kv_ref, tri, out_ref, cum_ref, rows, blocks):
    span = 2 * rows
    at_once = 2
    causal = (
        lax.broadcasted_iota(jnp.int32, (rows, span), 1)
        <= lax.broadcasted_iota(jnp.int32, (rows, span), 0) + half * rows
    )
    place = pl.multiple_of(half * rows, rows)

    def one_block(block, slot, state):
        keys = pl.ds(pl.multiple_of(block * span, span), span)
        gate = kv_ref[keys, 0:HEAD].astype(f32)
        values = kv_ref[keys, HEAD:]
        key_in = room / (1.0 + jnp.exp(gate))
        log_forget = jnp.log(1.0 - key_in)
        cum = mm(tri, jnp.concatenate(halves(log_forget), 0))
        last = cum[span - 1 : span, :]
        cum_ref[slot] = cum
        own_cum = cum_ref[slot, pl.ds(place, rows), :]
        queries = q_ref[pl.ds(pl.multiple_of(block * rows, rows), rows), :].astype(f32)
        q_dec = (queries * jnp.exp(own_cum)).astype(bf16)
        k_inv = (key_in * jnp.exp(-cum)).astype(bf16)
        k_end = (key_in * jnp.exp(last - cum)).astype(bf16)
        scores = jnp.where(causal, mm_t(q_dec, k_inv), 0.0).astype(bf16)
        raw = mm(scores, values) + mm_t(q_dec, state.astype(bf16))
        fresh = lax.dot_general(values, k_end, (((0,), (0,)), ((), ())), preferred_element_type=f32)
        scale = lax.rsqrt(jnp.mean(raw * raw, axis=1, keepdims=True) + NORM_EPS)
        out_ref[block] = (raw * scale * gain).astype(bf16)
        return state * jnp.exp(last) + fresh

    def some_blocks(step, state):
        for slot in range(at_once):
            state = one_block(step * at_once + slot, slot, state)
        return state

    lax.fori_loop(0, blocks // at_once, some_blocks, jnp.zeros((HEAD, HEAD), f32))


def mixer_kernel(gain_ref, query_ref, mine_ref, other_ref, *refs):
    out_ref, q_ref, kv_ref, acc_ref, carry_ref, cum_ref, sums_ref = refs
    blocks, rows, _ = out_ref.shape
    span = 2 * rows
    place, half = lax.axis_index("sp"), lax.axis_index("tp")
    head, _, is_attn = place_of_head()

    def settle(k, _):
        slot = jnp.where(k < 7, k, jnp.where(k < MOST, 22 - k, k - 5))
        block = (place + slot) % blocks
        own = pl.ds(pl.multiple_of(k * rows, rows), rows)
        q_ref[pl.ds(pl.multiple_of(block * rows, rows), rows), :] = query_ref[own, :]
        at = pl.multiple_of((2 * block + half) * rows, rows)
        kv_ref[pl.ds(at, rows), :] = mine_ref[own, :]
        at = pl.multiple_of((2 * block + 1 - half) * rows, rows)
        kv_ref[pl.ds(at, rows), :] = other_ref[own, :]
        return 0

    lax.fori_loop(0, blocks, settle, 0)
    used = blocks * rows
    holds = holder_of(head) == half
    parts = jnp.where(
        holds, mine_ref[used : used + 8, :].astype(f32), other_ref[used : used + 8, :].astype(f32)
    )
    params = parts[0:1, :] + parts[1:2, :] + parts[2:3, :]
    room, offset = params[:, :HEAD], params[:, HEAD:]
    down = lax.broadcasted_iota(jnp.int32, (span, span), 0)
    across = lax.broadcasted_iota(jnp.int32, (span, span), 1)

    @pl.when(is_attn)
    def _():
        later = jnp.where(down > across, 1.0, 0.0).astype(bf16)
        for k in range(2):
            sums_ref[k * span : (k + 1) * span, 0:span] = later
            sums_ref[k * span : (k + 1) * span, span:] = jnp.ones((span, span), bf16)
        stick_body(half, offset, q_ref, kv_ref, sums_ref, out_ref, acc_ref, carry_ref, rows, blocks)

    @pl.when(jnp.logical_not(is_attn))
    def _():
        upto = jnp.where(down >= across, 1.0, 0.0).astype(bf16)
        tri = jnp.concatenate([upto, upto], 1)
        recur_body(half, room, gain_ref[...], q_ref, kv_ref, tri, out_ref, cum_ref, rows, blocks)


def output_kernel(heads_ref, *refs):
    out_ref = refs[-1]
    fs = lax.axis_size("fs")
    x, half = lax.axis_index("fs"), lax.axis_index("tp")
    pieces = refs[:fs], refs[fs : 2 * fs]
    width = pieces[0][0].shape[1]
    depth = heads_ref.shape[0] // 2 * HEAD
    heads = heads_ref.shape[0] // 2
    each = heads // 2
    sides = []
    for core in range(2):
        first = each * (half if core == 0 else 1 - half)
        sides.append(
            jnp.concatenate(
                [heads_ref[kind * heads + first + k] for kind in range(2) for k in range(each)], 1
            )
        )
    for step in range(fs):
        total = sum(mm(sides[core], pieces[core][step][0:depth, :]) for core in range(2))
        at = pl.multiple_of((x + step) % fs * width, width)
        out_ref[:, pl.ds(at, width)] = total.astype(bf16)


SLOTS = (0, 1, 2, 3, 4, 5, 6, 15, 14, 13, 12, 11, 7, 8, 9, 10)
MOST = 12
PARAM_ROWS = 16

MIB = 1 << 20


def limit(mib):
    return pltpu.CompilerParams(vmem_limit_bytes=mib * MIB)


def resident(arrays):
    return [pltpu.with_memory_space_constraint(a, pltpu.VMEM) for a in arrays]


def left_out(arrays):
    return [pltpu.with_memory_space_constraint(a, pltpu.HBM) for a in arrays]


whole = pl.BlockSpec(memory_space=pltpu.VMEM)
scalar = pl.BlockSpec(memory_space=pltpu.SMEM)
outside = pl.BlockSpec(memory_space=pltpu.HBM)


def place_of_head():
    heads = lax.axis_size("sp") // 2
    place = lax.axis_index("sp")
    head = place % heads
    return head, head % (heads // lax.axis_size("tp")), place < heads


def holder_of(head):
    return head // (lax.axis_size("sp") // 2 // lax.axis_size("tp"))


def body(
    tokens,
    mix_gain,
    attn_query,
    attn_key,
    attn_value,
    rec_query,
    rec_forget,
    rec_input,
    break_offset,
    forget_room,
    out_gain,
    out_attn,
    out_rec,
):
    sp, fs, tp = (lax.axis_size(a) for a in ("sp", "fs", "tp"))
    t = lax.axis_index("tp")
    _, _, _ = place_of_head()

    rows = tokens.shape[1] // tp
    half_width = tokens.shape[2]
    own = tokens[0]
    near = lax.dynamic_slice_in_dim(own, t * rows, rows, 0)
    far = swap(lax.dynamic_slice_in_dim(own, (1 - t) * rows, rows, 0))

    depth, wide = out_attn.shape
    shape = jax.ShapeDtypeStruct((3 * HEAD, attn_query.shape[0]), bf16)
    pick = pl.pallas_call(
        columns_kernel,
        out_shape=shape,
        in_specs=[outside] * 6,
        out_specs=whole,
        scratch_shapes=[
            pltpu.VMEM((3, attn_query.shape[0], HEAD), bf16),
            pltpu.SemaphoreType.DMA((3,)),
        ],
        compiler_params=limit(6),
        name="columns",
    )
    columns = pick(*left_out([attn_query, attn_key, attn_value, rec_query, rec_forget, rec_input]))
    columns_other = swap(columns)
    pack = pl.pallas_call(
        pack_kernel,
        out_shape=jax.ShapeDtypeStruct((2 * depth + shape.shape[0], wide), bf16),
        in_specs=[whole, whole, outside, outside],
        out_specs=whole,
        scratch_shapes=[pltpu.SemaphoreType.DMA((2,))],
        compiler_params=limit(8),
        name="pack",
    )
    pack = pack(*resident([columns, columns_other]), *left_out([out_attn, out_rec]))
    from_prev, from_next = shift(pack, "fs", 1), shift(pack, "fs", -1)
    far_columns = from_prev[2 * depth :]
    far_columns = shift(far_columns, "fs", 1)
    from_far = shift(from_prev, "fs", 1)
    mine = [pack, from_next, from_far, from_prev]
    other_own, other_next, other_prev = swap(pack), swap(from_next), swap(from_prev)
    other_far = swap(from_far)
    other = [other_own, other_next, other_far, other_prev]

    last = sp // 2
    near_blocks, far_blocks = {0: near}, {0: far}
    ahead = [near, far]
    behind = [near, far]
    for hop in range(1, last + 1):
        for k, store in enumerate((near_blocks, far_blocks)):
            if hop < last or k == 0:
                ahead[k] = shift(ahead[k], "sp", 1)
                store[sp - hop] = ahead[k]
            if hop < last or k == 1:
                behind[k] = shift(behind[k], "sp", -1)
                store[hop] = behind[k]

    def project(done, slots, earlier):
        count = len(slots) * rows
        extra = PARAM_ROWS if done else 0
        return pl.pallas_call(
            functools.partial(project_kernel, done),
            out_shape=(
                jax.ShapeDtypeStruct((done + count, HEAD), bf16),
                jax.ShapeDtypeStruct((done + count + extra, 2 * HEAD), bf16),
            ),
            in_specs=[whole, scalar] + [whole] * (1 + len(earlier) + fs + 2 * len(slots)),
            out_specs=(whole, whole),
            scratch_shapes=[pltpu.VMEM((count, 2 * half_width), bf16)],
            compiler_params=limit(12),
            name="project",
        )(
            mix_gain[None, :],
            break_offset,
            forget_room,
            *resident(earlier),
            *resident([pack, from_next, far_columns, from_prev]),
            *resident([near_blocks[s] for s in slots]),
            *resident([far_blocks[s] for s in slots]),
        )

    most = project(0, SLOTS[:MOST], [])
    query, pair = project(MOST * rows, SLOTS[MOST:], most)
    pair_other = swap(pair)

    span = rows * tp
    mixed_heads = pl.pallas_call(
        mixer_kernel,
        out_shape=jax.ShapeDtypeStruct((sp, rows, HEAD), bf16),
        in_specs=[whole] * 4,
        out_specs=whole,
        scratch_shapes=[
            pltpu.VMEM((sp * rows, HEAD), bf16),
            pltpu.VMEM((sp * span, 2 * HEAD), bf16),
            pltpu.VMEM((4 * rows, HEAD), f32),
            pltpu.VMEM((4 * rows, HEAD), f32),
            pltpu.VMEM((2, span, HEAD), f32),
            pltpu.VMEM((2 * span, 2 * span), bf16),
        ],
        compiler_params=limit(12),
        name="mixer",
    )(out_gain[None, :], *resident([query, pair, pair_other]))

    arrived = lax.all_to_all(mixed_heads, "sp", split_axis=0, concat_axis=0, tiled=True)
    mixed = pl.pallas_call(
        output_kernel,
        out_shape=jax.ShapeDtypeStruct((rows, fs * out_attn.shape[1]), bf16),
        in_specs=[whole] * (1 + 2 * fs),
        out_specs=whole,
        compiler_params=limit(16),
        name="output",
    )(*resident([arrived, *mine, *other]))
    return mixed[None]


def solution(mesh):
    placed = (
        P(("grp", "fs"), "sp", "tp"),
        P(),
        P("fs", "tp"),
        P("fs", "tp"),
        P("fs", "tp"),
        P("fs", "tp"),
        P("fs", "tp"),
        P("fs", "tp"),
        P("tp"),
        P("tp", None),
        P(),
        P("tp", "fs"),
        P("tp", "fs"),
    )
    return jax.shard_map(
        body,
        mesh=mesh,
        in_specs=placed,
        out_specs=P(("grp", "fs"), ("sp", "tp"), None),
        check_vma=False,
    )
```

```python
import functools
import math

import jax
import jax.numpy as jnp
from jax import lax
from jax.experimental import pallas as pl
from jax.experimental.pallas import tpu as pltpu
from jax.sharding import PartitionSpec as P


HEAD = 128
NORM_EPS = 1e-06
LOG2E = 1.4426950408889634

f32 = jnp.float32
bf16 = jnp.bfloat16


def mm(a, b):
    return lax.dot_general(a, b, (((1,), (0,)), ((), ())), preferred_element_type=f32)


def mm_t(a, b):
    return lax.dot_general(a, b, (((1,), (1,)), ((), ())), preferred_element_type=f32)


def halves(x):
    top = x.astype(bf16)
    return top, (x - top.astype(f32)).astype(bf16)


def ring(size, step):
    return [(k, (k + step) % size) for k in range(size)]


def shift(x, axis, step):
    return lax.ppermute(x, axis, ring(lax.axis_size(axis), step))


def swap(x):
    return lax.ppermute(x, "tp", [(0, 1), (1, 0)])


def columns_kernel(*refs):
    attn, rec = refs[0:3], refs[3:6]
    out_ref, sems = refs[6:]
    _, local, is_attn = place_of_head()
    at = pl.ds(pl.multiple_of(local * HEAD, HEAD), HEAD)

    def columns(sources):
        copies = [
            pltpu.make_async_copy(
                sources[k].at[:, at], out_ref.at[:, k * HEAD : (k + 1) * HEAD], sems.at[k]
            )
            for k in range(3)
        ]
        for copy in copies:
            copy.start()
        for copy in copies:
            copy.wait()

    @pl.when(is_attn)
    def _():
        columns(attn)

    @pl.when(jnp.logical_not(is_attn))
    def _():
        columns(rec)


def pack_kernel(mine_ref, other_ref, out_attn, out_rec, pack_ref, sems):
    rows = out_attn.shape[0]
    copies = [
        pltpu.make_async_copy(out_attn, pack_ref.at[0:rows, :], sems.at[0]),
        pltpu.make_async_copy(out_rec, pack_ref.at[rows : 2 * rows, :], sems.at[1]),
    ]
    for copy in copies:
        copy.start()
    head, _, _ = place_of_head()
    holds = holder_of(head) == lax.axis_index("tp")

    used = mine_ref.shape[1]
    pack_ref[2 * rows :, used:] = jnp.zeros((mine_ref.shape[0], pack_ref.shape[1] - used), bf16)

    @pl.when(holds)
    def _():
        pack_ref[2 * rows :, :used] = mine_ref[...]

    @pl.when(jnp.logical_not(holds))
    def _():
        pack_ref[2 * rows :, :used] = other_ref[...]

    for copy in copies:
        copy.wait()


def project_kernel(done, gain_ref, offset_ref, room_ref, *refs):
    fs = lax.axis_size("fs")
    query_ref, pair_ref, norm_ref = refs[-3:]
    if done:
        query_ref[0:done, :] = refs[0][...]
        pair_ref[0:done, :] = refs[1][...]
        refs = refs[2:]
    packs, refs = refs[:fs], refs[fs:]
    count = (len(refs) - 3) // 2
    near, far = refs[:count], refs[count : 2 * count]
    rows, half = near[0].shape
    each = near[0].shape[1] * 2 // fs
    x, t = lax.axis_index("fs"), lax.axis_index("tp")
    _, local, _ = place_of_head()
    at_a = pl.ds(pl.multiple_of(t * half, half), half)
    at_b = pl.ds(pl.multiple_of((1 - t) * half, half), half)
    for k in range(count):
        own = slice(k * rows, (k + 1) * rows)
        norm_ref[own, at_a] = near[k][...]
        norm_ref[own, at_b] = far[k][...]
    gain = gain_ref[...]

    def normalize(k, _):
        own = pl.ds(pl.multiple_of(k * rows, rows), rows)
        value = norm_ref[own, :].astype(f32)
        total = jnp.sum(value * value, axis=1, keepdims=True)
        factor = lax.rsqrt(total * (1.0 / (2 * half)) + NORM_EPS)
        norm_ref[own, :] = (value * factor * gain).astype(bf16)
        return 0

    lax.fori_loop(0, count, normalize, 0)
    group = 2 * rows

    def multiply(k, _):
        own = pl.ds(pl.multiple_of(k * group, group), group)
        product = 0.0
        for step in range(fs):
            at = pl.ds(pl.multiple_of((x + step) % fs * each, each), each)
            weight = packs[step][packs[step].shape[0] - each :, 0 : 3 * HEAD]
            product += mm(norm_ref[own, at], weight)
        product = product.astype(bf16)
        to = pl.ds(pl.multiple_of(done + k * group, group), group)
        query_ref[to, :] = product[:, :HEAD]
        pair_ref[to, :] = product[:, HEAD:]
        return 0

    lax.fori_loop(0, count * rows // group, multiply, 0)
    if not done:
        return
    offset = jnp.full((1, HEAD), offset_ref[local], f32)
    rest = jnp.concatenate([room_ref[pl.ds(local, 1), :], offset], 1)
    parts = []
    for _ in range(3):
        parts.append(rest.astype(bf16).astype(f32))
        rest = rest - parts[-1]
    used = done + count * rows
    pad = jnp.zeros((PARAM_ROWS - 3, 2 * HEAD), f32)
    pair_ref[used : used + PARAM_ROWS, :] = jnp.concatenate(parts + [pad], 0).astype(bf16)


def stick_body(half, offset, q_ref, kv_ref, sums_ref, out_ref, acc_ref, carry_ref, rows, blocks):
    tile = 4
    span = 2 * rows
    factor = LOG2E / math.sqrt(HEAD)
    offset = jnp.concatenate([offset * LOG2E] * tile, 1)
    strict = (
        lax.broadcasted_iota(jnp.int32, (rows, span), 1)
        < lax.broadcasted_iota(jnp.int32, (rows, span), 0) + half * rows
    )

    def keys_of(group):
        return pl.ds(pl.multiple_of(group * (tile * span), tile * span), tile * span)

    def attend(queries, group, carry, diagonal):
        keys = keys_of(group)
        z = mm_t(queries, kv_ref[keys, 0:HEAD]) * factor + offset
        tail = jnp.log(1.0 + jnp.exp2(-jnp.abs(z))) * LOG2E
        drop = jnp.maximum(z, 0.0) + tail
        take = jnp.minimum(z, 0.0) - tail
        parts = [None] * tile
        for n in reversed(range(tile)):
            across = slice(n * span, (n + 1) * span)
            skip = n * rows if diagonal else 0
            this = drop[skip:, across]
            if diagonal:
                first = jnp.where(strict, this[:rows], 0.0)
                this = jnp.concatenate([first, this[rows:]], 0) if n < tile - 1 else first
            both = mm(jnp.concatenate(halves(this), 1), sums_ref[...])
            stick = jnp.exp2(take[skip:, across] - both[:, :span] - carry[skip:])
            total = both[:, span:]
            if diagonal:
                first = jnp.where(strict, stick[:rows], 0.0)
                stick = jnp.concatenate([first, stick[rows:]], 0) if n < tile - 1 else first
            stick = stick.astype(bf16)
            if skip:
                stick = jnp.concatenate([jnp.zeros((skip, span), bf16), stick], 0)
                total = jnp.concatenate([jnp.zeros((skip, span), f32), total], 0)
            parts[n] = stick
            carry = carry + total
        return mm(jnp.concatenate(parts, 1), kv_ref[keys, HEAD:]), carry

    def query_tile(index, _):
        own = pl.ds(pl.multiple_of(index * (tile * rows), tile * rows), tile * rows)
        start = jnp.zeros((tile * rows, span), f32)
        acc_ref[...], carry_ref[...] = attend(q_ref[own, :], index, start, True)

        def earlier(step, _):
            out, carry = attend(q_ref[own, :], index - 1 - step, carry_ref[...], False)
            acc_ref[...] += out
            carry_ref[...] = carry
            return 0

        lax.fori_loop(0, index, earlier, 0)
        for n in range(tile):
            out_ref[index * tile + n] = acc_ref[n * rows : (n + 1) * rows, :].astype(bf16)
        return 0

    lax.fori_loop(0, blocks // tile, query_tile, 0)


def recur_body(half, room, gain, q_ref, kv_ref, tri, out_ref, cum_ref, rows, blocks):
    span = 2 * rows
    at_once = 2
    causal = (
        lax.broadcasted_iota(jnp.int32, (rows, span), 1)
        <= lax.broadcasted_iota(jnp.int32, (rows, span), 0) + half * rows
    )
    place = pl.multiple_of(half * rows, rows)

    def one_block(block, slot, state):
        keys = pl.ds(pl.multiple_of(block * span, span), span)
        gate = kv_ref[keys, 0:HEAD].astype(f32)
        values = kv_ref[keys, HEAD:]
        key_in = room / (1.0 + jnp.exp(gate))
        log_forget = jnp.log(1.0 - key_in)
        cum = mm(tri, jnp.concatenate(halves(log_forget), 0))
        last = cum[span - 1 : span, :]
        cum_ref[slot] = cum
        own_cum = cum_ref[slot, pl.ds(place, rows), :]
        queries = q_ref[pl.ds(pl.multiple_of(block * rows, rows), rows), :].astype(f32)
        q_dec = (queries * jnp.exp(own_cum)).astype(bf16)
        k_inv = (key_in * jnp.exp(-cum)).astype(bf16)
        k_end = (key_in * jnp.exp(last - cum)).astype(bf16)
        scores = jnp.where(causal, mm_t(q_dec, k_inv), 0.0).astype(bf16)
        raw = mm(scores, values) + mm_t(q_dec, state.astype(bf16))
        fresh = lax.dot_general(values, k_end, (((0,), (0,)), ((), ())), preferred_element_type=f32)
        scale = lax.rsqrt(jnp.mean(raw * raw, axis=1, keepdims=True) + NORM_EPS)
        out_ref[block] = (raw * scale * gain).astype(bf16)
        return state * jnp.exp(last) + fresh

    def some_blocks(step, state):
        for slot in range(at_once):
            state = one_block(step * at_once + slot, slot, state)
        return state

    lax.fori_loop(0, blocks // at_once, some_blocks, jnp.zeros((HEAD, HEAD), f32))


def mixer_kernel(gain_ref, query_ref, mine_ref, other_ref, *refs):
    out_ref, q_ref, kv_ref, acc_ref, carry_ref, cum_ref, sums_ref = refs
    blocks, rows, _ = out_ref.shape
    span = 2 * rows
    place, half = lax.axis_index("sp"), lax.axis_index("tp")
    head, _, is_attn = place_of_head()

    def settle(k, _):
        slot = jnp.where(k < 7, k, jnp.where(k < MOST, 22 - k, k - 5))
        block = (place + slot) % blocks
        own = pl.ds(pl.multiple_of(k * rows, rows), rows)
        q_ref[pl.ds(pl.multiple_of(block * rows, rows), rows), :] = query_ref[own, :]
        at = pl.multiple_of((2 * block + half) * rows, rows)
        kv_ref[pl.ds(at, rows), :] = mine_ref[own, :]
        at = pl.multiple_of((2 * block + 1 - half) * rows, rows)
        kv_ref[pl.ds(at, rows), :] = other_ref[own, :]
        return 0

    lax.fori_loop(0, blocks, settle, 0)
    used = blocks * rows
    holds = holder_of(head) == half
    parts = jnp.where(
        holds, mine_ref[used : used + 8, :].astype(f32), other_ref[used : used + 8, :].astype(f32)
    )
    params = parts[0:1, :] + parts[1:2, :] + parts[2:3, :]
    room, offset = params[:, :HEAD], params[:, HEAD:]
    down = lax.broadcasted_iota(jnp.int32, (span, span), 0)
    across = lax.broadcasted_iota(jnp.int32, (span, span), 1)

    @pl.when(is_attn)
    def _():
        later = jnp.where(down > across, 1.0, 0.0).astype(bf16)
        for k in range(2):
            sums_ref[k * span : (k + 1) * span, 0:span] = later
            sums_ref[k * span : (k + 1) * span, span:] = jnp.ones((span, span), bf16)
        stick_body(half, offset, q_ref, kv_ref, sums_ref, out_ref, acc_ref, carry_ref, rows, blocks)

    @pl.when(jnp.logical_not(is_attn))
    def _():
        upto = jnp.where(down >= across, 1.0, 0.0).astype(bf16)
        tri = jnp.concatenate([upto, upto], 1)
        recur_body(half, room, gain_ref[...], q_ref, kv_ref, tri, out_ref, cum_ref, rows, blocks)


def output_kernel(heads_ref, *refs):
    out_ref = refs[-1]
    fs = lax.axis_size("fs")
    x, half = lax.axis_index("fs"), lax.axis_index("tp")
    pieces = refs[:fs], refs[fs : 2 * fs]
    width = pieces[0][0].shape[1]
    depth = heads_ref.shape[0] // 2 * HEAD
    heads = heads_ref.shape[0] // 2
    each = heads // 2
    sides = []
    for core in range(2):
        first = each * (half if core == 0 else 1 - half)
        sides.append(
            jnp.concatenate(
                [heads_ref[kind * heads + first + k] for kind in range(2) for k in range(each)], 1
            )
        )
    for step in range(fs):
        total = sum(mm(sides[core], pieces[core][step][0:depth, :]) for core in range(2))
        at = pl.multiple_of((x + step) % fs * width, width)
        out_ref[:, pl.ds(at, width)] = total.astype(bf16)


SLOTS = (0, 1, 2, 3, 4, 5, 6, 15, 14, 13, 12, 11, 7, 8, 9, 10)
MOST = 12
PARAM_ROWS = 16

MIB = 1 << 20


def limit(mib):
    return pltpu.CompilerParams(vmem_limit_bytes=mib * MIB)


def resident(arrays):
    return [pltpu.with_memory_space_constraint(a, pltpu.VMEM) for a in arrays]


def left_out(arrays):
    return [pltpu.with_memory_space_constraint(a, pltpu.HBM) for a in arrays]


whole = pl.BlockSpec(memory_space=pltpu.VMEM)
scalar = pl.BlockSpec(memory_space=pltpu.SMEM)
outside = pl.BlockSpec(memory_space=pltpu.HBM)


def place_of_head():
    heads = lax.axis_size("sp") // 2
    place = lax.axis_index("sp")
    head = place % heads
    return head, head % (heads // lax.axis_size("tp")), place < heads


def holder_of(head):
    return head // (lax.axis_size("sp") // 2 // lax.axis_size("tp"))


def body(
    tokens,
    mix_gain,
    attn_query,
    attn_key,
    attn_value,
    rec_query,
    rec_forget,
    rec_input,
    break_offset,
    forget_room,
    out_gain,
    out_attn,
    out_rec,
):
    sp, fs, tp = (lax.axis_size(a) for a in ("sp", "fs", "tp"))
    t = lax.axis_index("tp")
    _, _, _ = place_of_head()

    rows = tokens.shape[1] // tp
    half_width = tokens.shape[2]
    own = tokens[0]
    near = lax.dynamic_slice_in_dim(own, t * rows, rows, 0)
    far = swap(lax.dynamic_slice_in_dim(own, (1 - t) * rows, rows, 0))

    depth, wide = out_attn.shape
    shape = jax.ShapeDtypeStruct((attn_query.shape[0], 3 * HEAD), bf16)
    pick = pl.pallas_call(
        columns_kernel,
        out_shape=shape,
        in_specs=[outside] * 6,
        out_specs=whole,
        scratch_shapes=[
            pltpu.SemaphoreType.DMA((3,)),
        ],
        compiler_params=limit(6),
        name="columns",
    )
    columns = pick(*left_out([attn_query, attn_key, attn_value, rec_query, rec_forget, rec_input]))
    columns_other = swap(columns)
    pack = pl.pallas_call(
        pack_kernel,
        out_shape=jax.ShapeDtypeStruct((2 * depth + shape.shape[0], wide), bf16),
        in_specs=[whole, whole, outside, outside],
        out_specs=whole,
        scratch_shapes=[pltpu.SemaphoreType.DMA((2,))],
        compiler_params=limit(8),
        name="pack",
    )
    pack = pack(*resident([columns, columns_other]), *left_out([out_attn, out_rec]))
    from_prev, from_next = shift(pack, "fs", 1), shift(pack, "fs", -1)
    far_columns = from_prev[2 * depth :, : 3 * HEAD]
    far_columns = shift(far_columns, "fs", 1)
    from_far = shift(from_prev, "fs", 1)
    mine = [pack, from_next, from_far, from_prev]
    other_own, other_next, other_prev = swap(pack), swap(from_next), swap(from_prev)
    other_far = swap(from_far)
    other = [other_own, other_next, other_far, other_prev]

    last = sp // 2
    near_blocks, far_blocks = {0: near}, {0: far}
    ahead = [near, far]
    behind = [near, far]
    for hop in range(1, last + 1):
        for k, store in enumerate((near_blocks, far_blocks)):
            if hop < last or k == 0:
                ahead[k] = shift(ahead[k], "sp", 1)
                store[sp - hop] = ahead[k]
            if hop < last or k == 1:
                behind[k] = shift(behind[k], "sp", -1)
                store[hop] = behind[k]

    def project(done, slots, earlier):
        count = len(slots) * rows
        extra = PARAM_ROWS if done else 0
        return pl.pallas_call(
            functools.partial(project_kernel, done),
            out_shape=(
                jax.ShapeDtypeStruct((done + count, HEAD), bf16),
                jax.ShapeDtypeStruct((done + count + extra, 2 * HEAD), bf16),
            ),
            in_specs=[whole, scalar] + [whole] * (1 + len(earlier) + fs + 2 * len(slots)),
            out_specs=(whole, whole),
            scratch_shapes=[pltpu.VMEM((count, 2 * half_width), bf16)],
            compiler_params=limit(12),
            name="project",
        )(
            mix_gain[None, :],
            break_offset,
            forget_room,
            *resident(earlier),
            *resident([pack, from_next, far_columns, from_prev]),
            *resident([near_blocks[s] for s in slots]),
            *resident([far_blocks[s] for s in slots]),
        )

    most = project(0, SLOTS[:MOST], [])
    query, pair = project(MOST * rows, SLOTS[MOST:], most)
    pair_other = swap(pair)

    span = rows * tp
    mixed_heads = pl.pallas_call(
        mixer_kernel,
        out_shape=jax.ShapeDtypeStruct((sp, rows, HEAD), bf16),
        in_specs=[whole] * 4,
        out_specs=whole,
        scratch_shapes=[
            pltpu.VMEM((sp * rows, HEAD), bf16),
            pltpu.VMEM((sp * span, 2 * HEAD), bf16),
            pltpu.VMEM((4 * rows, HEAD), f32),
            pltpu.VMEM((4 * rows, HEAD), f32),
            pltpu.VMEM((2, span, HEAD), f32),
            pltpu.VMEM((2 * span, 2 * span), bf16),
        ],
        compiler_params=limit(12),
        name="mixer",
    )(out_gain[None, :], *resident([query, pair, pair_other]))

    arrived = lax.all_to_all(mixed_heads, "sp", split_axis=0, concat_axis=0, tiled=True)
    mixed = pl.pallas_call(
        output_kernel,
        out_shape=jax.ShapeDtypeStruct((rows, fs * out_attn.shape[1]), bf16),
        in_specs=[whole] * (1 + 2 * fs),
        out_specs=whole,
        compiler_params=limit(16),
        name="output",
    )(*resident([arrived, *mine, *other]))
    return mixed[None]


def solution(mesh):
    placed = (
        P(("grp", "fs"), "sp", "tp"),
        P(),
        P("fs", "tp"),
        P("fs", "tp"),
        P("fs", "tp"),
        P("fs", "tp"),
        P("fs", "tp"),
        P("fs", "tp"),
        P("tp"),
        P("tp", None),
        P(),
        P("tp", "fs"),
        P("tp", "fs"),
    )
    return jax.shard_map(
        body,
        mesh=mesh,
        in_specs=placed,
        out_specs=P(("grp", "fs"), ("sp", "tp"), None),
        check_vma=False,
    )
```
